32 devices in a mesh: sp: 8 (over z, y), tp: 4 (over x, core).
Axes of the slice: x: 2, y: 2, z: 4, core: 2. Of those that a mesh axis runs over, the one named last changes fastest.
Arguments:
- queries_nope: bfloat16 [3072, 8, 128], P('sp', 'tp'), may hold values from -9 to 9
- queries_rope: bfloat16 [3072, 8, 64], P('sp', 'tp'), may hold values from -6 to 6
- latent: bfloat16 [3072, 512], P('sp'), may hold values from -8 to 8, as said below
- rope_key: bfloat16 [3072, 64], P('sp'), may hold values from -6 to 6
- latent_gain: float32 [512], replicated, may hold values from 0.1 to 1.9
- key_up: bfloat16 [512, 1024], P(None, 'tp'), may hold values from -0.25 to 0.25
- value_up: bfloat16 [512, 1024], P(None, 'tp'), may hold values from -0.25 to 0.25
- out_proj: bfloat16 [1024, 2048], P('tp'), may hold values from -0.75 to 0.75
- stream: bfloat16 [3072, 2048], P(('sp', 'tp')), may hold values from -6 to 6
- mix_gain: float32 [2048], replicated, may hold values from 0.1 to 1.9
- w_gate: bfloat16 [2048, 3072], P('sp', 'tp'), may hold values from -0.125 to 0.125
- w_up: bfloat16 [2048, 3072], P('sp', 'tp'), may hold values from -0.125 to 0.125
- w_down: bfloat16 [3072, 2048], P('tp', 'sp'), may hold values from -0.4375 to 0.4375
- mlp_gain: float32 [2048], replicated, may hold values from 0.1 to 1.9
Outputs:
- result: bfloat16 [3072, 2048], P(('sp', 'tp'))
The draws below stay inside these ranges and needn't reach their ends.
Inputs may be any that keep to these rules, and one draw needn't show every extreme that they name: latent rows carry a mean vector that changes from one eighth of the sequence to the next.
All inputs are finite; a program needn't handle non-finite values.
Results may differ from the reference program's by a relative error of at most 0.017.
Values may be sent and summed in bfloat16 or wider, within the bound.
A program may use at most 192 MiB of HBM per device.

```python
import math
import jax
import jax.numpy as jnp
from jax import lax

D = 2048
HEADS = 8
HEAD = 128
ROPE = 64
LATENT = 512
FF = 3072
SEQ = 3072


def draw_latent(key, part):
    base = jax.random.fold_in(key, 11)
    noise_key, centre_key, factor_key = jax.random.split(base, 3)
    places = jnp.arange(SEQ, dtype=jnp.int32)
    segment = places * 8 // SEQ
    centres = jax.random.normal(centre_key, (8, LATENT), jnp.float32) * 1.5
    noise = jax.random.normal(noise_key, (SEQ, LATENT), jnp.float32)
    return jnp.clip(noise + centres[segment], -8.0, 8.0).astype(jnp.bfloat16)


def rope_pair(key):
    base = jax.random.fold_in(key, 23)
    first_key, second_key, third_key = jax.random.split(base, 3)
    key_part = jnp.clip(jax.random.normal(first_key, (SEQ, ROPE), jnp.float32), -6.0, 6.0)
    query_part = jnp.clip(jax.random.normal(second_key, (SEQ, HEADS, ROPE), jnp.float32), -6.0, 6.0)
    return (query_part.astype(jnp.bfloat16), key_part.astype(jnp.bfloat16))


def draw_queries_rope(key, part):
    return rope_pair(key)[0]


def draw_rope_key(key, part):
    return rope_pair(key)[1]


def levels(own_key, dims, cuts, least, high):
    def one(dim, shards_of):
        heights = jax.random.uniform(jax.random.fold_in(jax.random.fold_in(own_key, 6), dim), (shards_of,), jnp.float32, least / len(cuts), high / len(cuts))
        return jnp.repeat(jnp.exp(heights), dims[dim] // shards_of).reshape((-1,) + (1,) * (len(dims) - dim - 1))

    factor_of = one(*cuts[0])
    for cut in cuts[1:]:
        factor_of = factor_of * one(*cut)
    return factor_of


def normal_values(own_key, dims, scale, reach, shards=(), held_as=jnp.bfloat16):
    loudness = levels(own_key, dims, shards, -0.22, 0.18) if shards else 1.0
    drawn = jax.random.normal(own_key, dims, jnp.float32) * scale * loudness
    return jnp.minimum(jnp.maximum(drawn, -reach), reach).astype(held_as)


def setup_inputs(seed: int = 0) -> dict:
    seeds = jax.random.split(jax.random.key(seed), 15)
    queries_nope = normal_values(seeds[0], (SEQ, HEADS, HEAD), 3.0, 9.0, ((0, 8), (1, 4)))
    queries_rope = draw_queries_rope(jax.random.fold_in(seeds[14], 71), 0)
    latent = draw_latent(jax.random.fold_in(seeds[14], 71), 0)
    rope_key = draw_rope_key(jax.random.fold_in(seeds[14], 71), 0)
    latent_gain = jnp.clip(1.0 + 0.18 * jax.random.normal(seeds[4], (LATENT,), jnp.float32), 0.1, 1.9)
    key_up = normal_values(seeds[5], (LATENT, HEADS * HEAD), LATENT ** -0.5, 0.25, ((1, 4),))
    value_up = normal_values(seeds[6], (LATENT, HEADS * HEAD), LATENT ** -0.5, 0.25, ((1, 4),))
    out_proj = normal_values(seeds[7], (HEADS * HEAD, D), (HEADS * HEAD // 16) ** -0.5, 0.75, ((0, 4),))
    stream = normal_values(seeds[8], (SEQ, D), 1.0, 6.0, ((0, 32),))
    mix_gain = jnp.clip(1.0 + 0.18 * jax.random.normal(seeds[9], (D,), jnp.float32), 0.1, 1.9)
    w_gate = normal_values(seeds[10], (D, FF), D ** -0.5, 0.125, ((0, 8), (1, 4)))
    w_up = normal_values(seeds[11], (D, FF), D ** -0.5, 0.125, ((0, 8), (1, 4)))
    w_down = normal_values(seeds[12], (FF, D), (FF // 16) ** -0.5, 0.4375, ((0, 4), (1, 8)))
    mlp_gain = jnp.clip(1.0 + 0.18 * jax.random.normal(seeds[13], (D,), jnp.float32), 0.1, 1.9)
    return dict(queries_nope=queries_nope, queries_rope=queries_rope, latent=latent, rope_key=rope_key, latent_gain=latent_gain, key_up=key_up, value_up=value_up, out_proj=out_proj, stream=stream, mix_gain=mix_gain, w_gate=w_gate, w_up=w_up, w_down=w_down, mlp_gain=mlp_gain)


theta_base = 10000.0
residual_weight = 8.0 ** 0.25
norm_floor = 1.0
big_negative = -1e+30

def rotate(vector, first_row):
    half = vector.shape[-1] // 2
    rates = theta_base ** (-2.0 * jnp.arange(half, dtype=jnp.float32) / vector.shape[-1])
    places = (first_row + jnp.arange(vector.shape[0], dtype=jnp.int32)).astype(jnp.float32)
    angle = places[:, None] * rates[None, :]
    angle = angle.reshape((vector.shape[0],) + (1,) * (vector.ndim - 2) + (half,))
    cosine = jnp.cos(angle)
    sine = jnp.sin(angle)
    left = vector[..., :half]
    right = vector[..., half:]
    return jnp.concatenate([left * cosine - right * sine, left * sine + right * cosine], axis=-1)

def latent_norm(latent, latent_gain):
    wide = latent.astype(jnp.float32)
    factor = lax.rsqrt(lax.optimization_barrier(jnp.mean(wide * wide, axis=-1, keepdims=True)) + norm_floor)
    return (wide * factor * latent_gain).astype(jnp.bfloat16)

def layer_norm(values, gain):
    centre = lax.optimization_barrier(jnp.mean(values, axis=-1, keepdims=True))
    centred = values - centre
    spread = lax.optimization_barrier(jnp.mean(centred * centred, axis=-1, keepdims=True))
    return centred * lax.rsqrt(spread + norm_floor) * gain

def widen(array):
    return lax.optimization_barrier(array).astype(jnp.float32)

def reference(queries_nope, queries_rope, latent, rope_key, latent_gain, key_up, value_up, out_proj, stream, mix_gain, w_gate, w_up, w_down, mlp_gain):
    seq_len, head_count, head_dim = queries_nope.shape
    rope_dim = queries_rope.shape[2]
    query_turned = rotate(queries_rope.astype(jnp.float32), 0).astype(jnp.bfloat16)
    key_turned = rotate(rope_key.astype(jnp.float32), 0).astype(jnp.bfloat16)
    normed = latent_norm(latent, latent_gain)
    keys = jnp.dot(normed, key_up, preferred_element_type=jnp.float32).astype(jnp.bfloat16)
    keys = widen(keys).reshape(seq_len, head_count, head_dim)
    values_all = jnp.dot(normed, value_up, preferred_element_type=jnp.float32).astype(jnp.bfloat16)
    values_all = widen(values_all).reshape(seq_len, head_count, head_dim)
    key_wide = key_turned.astype(jnp.float32)
    scale = (head_dim + rope_dim) ** (-0.5)
    block = math.gcd(seq_len, 512)
    key_places = jnp.arange(seq_len, dtype=jnp.int32)

    def one_block(index):
        begin = (index * block).astype(jnp.int32)
        query_block = lax.dynamic_slice_in_dim(queries_nope, begin, block, 0).astype(jnp.float32)
        turned_block = lax.dynamic_slice_in_dim(query_turned, begin, block, 0).astype(jnp.float32)
        score = jnp.einsum('thd,shd->hts', query_block, keys) + jnp.einsum('thr,sr->hts', turned_block, key_wide)
        score = score * scale
        allowed = key_places[None, :] <= (begin + jnp.arange(block, dtype=jnp.int32))[:, None]
        score = jnp.where(allowed[None], score, big_negative)
        top = lax.optimization_barrier(jnp.max(score, axis=2, keepdims=True))
        powers = jnp.exp(score - top) * allowed[None]
        denominators = lax.optimization_barrier(jnp.sum(powers, axis=2))
        summed = jnp.einsum('hts,shd->thd', widen(powers.astype(jnp.bfloat16)), values_all)
        return (summed / denominators.T[:, :, None]).astype(jnp.bfloat16)
    blocks = lax.map(one_block, jnp.arange(seq_len // block, dtype=jnp.int32))
    attended = blocks.reshape(seq_len, head_count * head_dim)
    projected = jnp.dot(attended, out_proj, preferred_element_type=jnp.float32)
    mixed = layer_norm(residual_weight * stream.astype(jnp.float32) + projected, mix_gain).astype(jnp.bfloat16)
    gate_sum = jnp.dot(mixed, w_gate, preferred_element_type=jnp.float32)
    up_sum = jnp.dot(mixed, w_up, preferred_element_type=jnp.float32)
    hidden = (jax.nn.silu(gate_sum) * up_sum).astype(jnp.bfloat16)
    lowered = jnp.dot(hidden, w_down, preferred_element_type=jnp.float32)
    return layer_norm(residual_weight * mixed.astype(jnp.float32) + 0.5 * lowered, mlp_gain).astype(jnp.bfloat16)
```

```python
import functools
import math

import jax
import jax.numpy as jnp
from jax import lax
from jax.experimental import pallas as pl
from jax.experimental.pallas import tpu as pltpu
from jax.sharding import PartitionSpec as P

theta_base = 10000.0
residual_weight = 8.0**0.25
norm_floor = 1.0
big_negative = -1e30


def rotate(vector, first_row):
    half = vector.shape[-1] // 2
    rates = theta_base ** (-2.0 * jnp.arange(half, dtype=jnp.float32) / vector.shape[-1])
    places = (first_row + jnp.arange(vector.shape[0], dtype=jnp.int32)).astype(jnp.float32)
    angle = places[:, None] * rates[None, :]
    angle = angle.reshape((vector.shape[0],) + (1,) * (vector.ndim - 2) + (half,))
    cosine = jnp.cos(angle)
    sine = jnp.sin(angle)
    left = vector[..., :half]
    right = vector[..., half:]
    return jnp.concatenate([left * cosine - right * sine, left * sine + right * cosine], axis=-1)


def latent_norm(latent, latent_gain):
    wide = latent.astype(jnp.float32)
    factor = lax.rsqrt(jnp.mean(wide * wide, axis=-1, keepdims=True) + norm_floor)
    return (wide * factor * latent_gain).astype(jnp.bfloat16)


def layer_norm(values, gain):
    centre = jnp.mean(values, axis=-1, keepdims=True)
    centred = values - centre
    spread = jnp.mean(centred * centred, axis=-1, keepdims=True)
    return centred * lax.rsqrt(spread + norm_floor) * gain


mesh_id = pl.DeviceIdType.MESH
bf16 = jnp.bfloat16
f32 = jnp.float32


def layer_kernel(
    chain,
    teams,
    scale,
    qcat,
    latent_in,
    key_up,
    value_up,
    proj_in,
    stream,
    mix_gain,
    gate_in,
    up_in,
    down_in,
    mlp_gain,
    result,
    lat,
    gate,
    up,
    down,
    proj,
    heads_out,
    heads_in,
    share_out,
    share_in,
    rows,
    hidden,
    terms_out,
    mate_in,
    terms,
    x_first,
    z_first,
    x_relay,
    z_relay,
    x_last,
    z_last,
    wide,
    top,
    total,
    weighted,
    local_sem,
    lat_recv,
    lat_z,
    lat_y,
    lat_w,
    lat_next,
    lat_x,
    lat_m,
    w_recv,
    w_z,
    w_y,
    core_recv,
    core_send,
    share_recv,
    share_send,
    row_recv,
    row_send,
    mate_recv,
    mate_send,
    term_recv,
    term_send,
):
    sp = lax.axis_index("sp")
    t = lax.axis_index("tp")
    q = sp // 2
    p = sp % 2
    other = 1 - p
    half = t % 2
    column = t // 2
    columns = teams // 2
    mate = t + 1 - 2 * half
    layer = q % 2
    group = 2 * teams
    mine = half * teams + column * 2 + layer
    last = chain - 1
    head_count = qcat.shape[0]
    head_dim = value_up.shape[1] // head_count
    block_rows = qcat.shape[1]
    width = value_up.shape[0]
    part = block_rows // teams

    def place(pp, tt, qq=None):
        return ((q if qq is None else qq) * 2 + pp, tt)

    def across(step):
        return lax.rem(t + step, teams)

    def remote(source, target, send, recv, device):
        return pltpu.make_async_remote_copy(
            src_ref=source,
            dst_ref=target,
            send_sem=send,
            recv_sem=recv,
            device_id=device,
            device_id_type=mesh_id,
        )

    def pair_place(zz, tt):
        return place(p, tt, q - layer + zz)

    far_steps = range(2, teams, 2)
    barrier = pltpu.get_barrier_semaphore()
    peers = [place(p, t, lax.rem(q + d, chain)) for d in range(1, chain)]
    peers += [place(other, t), place(p, mate)]
    peers += [place(p, across(step)) for step in far_steps]
    peers += [pair_place(1 - layer, across(step)) for step in far_steps]
    for device in peers:
        pl.semaphore_signal(barrier, inc=1, device_id=device, device_id_type=mesh_id)
    with jax.named_scope("barrier"):
        pl.semaphore_wait(barrier, len(peers))

    def lat_to_z(qq):
        return remote(
            latent_in.at[t], lat.at[q, p, t], lat_z.at[qq], lat_recv.at[q, p, t], place(p, t, qq)
        )

    def lat_to_next(j):
        spot = lat.at[j, p, t]
        return remote(spot, spot, lat_next.at[j], lat_recv.at[j, p, t], place(p, t, q + 1))

    def lat_side(j, step):
        spot = lat.at[j, p, across(step)]
        return remote(
            spot, spot, lat_w.at[j, step], lat_recv.at[j, p, across(step)], place(other, t)
        )

    def turned(j):
        return (j % 2 == 1) & (j < q)

    def lat_own_y():
        return remote(
            latent_in.at[t], lat.at[q, p, t], lat_y.at[q], lat_recv.at[q, p, t], place(other, t)
        )

    def lat_to_y(j):
        spot = lat.at[j, p, t]
        return remote(spot, spot, lat_y.at[j], lat_recv.at[j, p, t], place(other, t))

    def lat_to_x(j, pp, step):
        spot = lat.at[j, pp, t]
        return remote(
            spot, spot, lat_x.at[j, pp, step], lat_recv.at[j, pp, t], place(p, across(step))
        )

    def lat_to_m(j, pp, tt):
        spot = lat.at[j, pp, tt]
        return remote(spot, spot, lat_m.at[j, pp, tt], lat_recv.at[j, pp, tt], place(p, mate))

    def lat_wait(j, pp, tt):
        spot = lat.at[j, pp, tt]
        with jax.named_scope("lat_wait"):
            remote(spot, spot, lat_y.at[0], lat_recv.at[j, pp, tt], place(p, mate)).wait_recv()

    stores = (gate, up, down)
    hidden_half = gate.shape[3]

    def piece(w, which):
        start = pl.multiple_of(which * hidden_half, 128)
        if w == 0:
            return gate_in.at[:, pl.ds(start, hidden_half)]
        if w == 1:
            return up_in.at[:, pl.ds(start, hidden_half)]
        return down_in.at[pl.ds(start, hidden_half), :]

    def w_to_z(w, qq):
        return remote(
            piece(w, qq % 2),
            stores[w].at[q, p],
            w_z.at[w, qq],
            w_recv.at[w, q, p],
            place(p, t, qq),
        )

    def w_own_y(w):
        return remote(
            piece(w, layer), stores[w].at[q, p], w_y.at[w, q], w_recv.at[w, q, p], place(other, t)
        )

    def w_to_y(w, j):
        spot = stores[w].at[j, p]
        return remote(spot, spot, w_y.at[w, j], w_recv.at[w, j, p], place(other, t))

    def w_wait(w, j, pp):
        spot = stores[w].at[j, pp]
        with jax.named_scope("w_wait"):
            remote(spot, spot, w_y.at[w, 0], w_recv.at[w, j, pp], place(p, mate)).wait_recv()

    def w_own(w):
        return pltpu.make_async_copy(piece(w, layer), stores[w].at[q, p], local_sem.at[1 + w])

    own_lat = pltpu.make_async_copy(latent_in, lat.at[q, p], local_sem.at[0])
    own_proj = pltpu.make_async_copy(proj_in, proj.at[half], local_sem.at[4])
    proj_mate = remote(proj_in, proj.at[half], core_send.at[0], core_recv.at[0], place(p, mate))

    def lat_own_to_z(act):
        for d in range(1, chain):

            takes = (q + d <= last) & (((q + d) % 2 == 0) | ((d == 1) & (layer == 0)))

            @pl.when(takes)
            def _():
                act(lat_to_z(q + d))

    def toward(w, near, act):
        for d in (1,) if near else range(last, 1, -1):

            @pl.when((layer == 0) & (q + d <= last))
            def _():
                act(w_to_z(w, q + d))

            @pl.when((layer == 1) & (q - d >= 0))
            def _():
                act(w_to_z(w, q - d))

    def away(w, act):
        for d in range(last, 0, -1):

            @pl.when((layer == 1) & (q + d <= last))
            def _():
                act(w_to_z(w, q + d))

            @pl.when((layer == 0) & (q - d >= 0))
            def _():
                act(w_to_z(w, q - d))

    def start(copy):
        copy.start()

    def sent(copy):
        copy.wait_send()

    own_lat.start()
    lat_own_to_z(start)

    @pl.when(p == 0)
    def _():
        lat_own_y().start()

    w_own_y(0).start()
    patient = q == last - 1

    def all_toward():
        toward(0, True, start)
        toward(0, False, start)
        toward(1, False, start)
        toward(1, True, start)
        toward(2, True, start)

    for w in range(3):
        away(w, start)

    @pl.when(jnp.logical_not(patient))
    def _():
        all_toward()

    for w in range(3):
        w_own(w).start()
    own_proj.start()
    proj_mate.start()

    top[...] = jnp.full_like(top, big_negative)
    total[...] = jnp.zeros_like(total)
    weighted[...] = jnp.zeros_like(weighted)

    def attend(j, pp, diagonal):
        block = lat[j, pp].reshape(block_rows, lat.shape[4])
        normed = block[:, :width]
        rotary = block[:, width:]
        keys = jnp.dot(normed, key_up[...], preferred_element_type=f32).astype(bf16)
        values = jnp.dot(normed, value_up[...], preferred_element_type=f32).astype(bf16)
        for h in range(head_count):
            span = slice(h * head_dim, (h + 1) * head_dim)
            both = jnp.concatenate([keys[:, span], rotary], axis=1)
            score = lax.dot_general(
                qcat[h], both, (((1,), (1,)), ((), ())), preferred_element_type=f32
            )
            if diagonal:
                down_rows = lax.broadcasted_iota(jnp.int32, score.shape, 0)
                over_columns = lax.broadcasted_iota(jnp.int32, score.shape, 1)
                score = jnp.where(over_columns <= down_rows, score, big_negative)
            old = top[h]
            new = jnp.maximum(old, jnp.max(score, axis=1, keepdims=True))
            powers = jnp.exp2(score * scale - new * scale)
            shrink = jnp.exp2((old - new) * scale)
            total[h] = total[h] * shrink + jnp.sum(powers, axis=1, keepdims=True)
            weighted[h] = weighted[h] * shrink + jnp.dot(
                powers.astype(bf16), values[:, span], preferred_element_type=f32
            )
            top[h] = new

    with jax.named_scope("own_lat"):
        own_lat.wait()
    with jax.named_scope("attend_own"):
        attend(q, p, True)

    def is_edge(j):
        return (j % 4 == 0) | (j % 4 == 3)

    def forward(w, kind):
        for j in range(chain):
            distant = q // 2 != j // 2
            if kind == 1:
                takes = (q // 2 == j // 2) & (q != j)
            elif is_edge(j) == (kind == 0):
                takes = distant
            else:
                continue

            @pl.when(takes)
            def _():
                w_wait(w, j, p)
                w_to_y(w, j).start()

    def lat_step(s, carry):
        a = q - s

        @pl.when(a >= 0)
        def _():
            lat_wait(a, p, t)
            lat_to_y(a).start()
            for step in far_steps:
                lat_to_x(a, p, step).start()
            lat_to_m(a, p, t).start()

            @pl.when(layer == 0)
            def _():
                lat_to_next(a).start()

        b = q - s + 1

        @pl.when((b >= 0) & ((s >= 2) | (p == 1)))
        def _():
            lat_wait(b, other, t)

            @pl.when(jnp.logical_not(turned(b)))
            def _():
                for step in far_steps:
                    lat_to_x(b, other, step).start()

            lat_to_m(b, other, t).start()

        @pl.when(s == 3)
        def _():
            w_own_y(1).start()

        @pl.when((s == 3) & patient)
        def _():
            all_toward()

        def block(j, pp):
            for i in range(columns):
                lat_wait(j, pp, 2 * i + 1 - half)
            with jax.named_scope("attend"):
                attend(j, pp, False)

        def stage(k, inner):
            e = q - s + 2 + k

            @pl.when((e >= 0) & ((s >= 4) | ((s == 3) & ((k == 0) | (p == 1)))))
            def _():
                block(e, jnp.where(k == 0, p, other))

            c = b + k
            side = jnp.where(k == 0, p, other)
            ready = (s >= 2) & ((k == 0) | (s >= 3) | (p == 1))

            @pl.when((c >= 0) & ready)
            def _():
                for step in far_steps:
                    lat_wait(c, side, across(step))

                    @pl.when(turned(c) & (k == 0))
                    def _():
                        lat_side(c, step).start()

                    lat_to_m(c, side, across(step)).start()

            return inner

        lax.fori_loop(0, 2, stage, 0)
        for turn, w, kind in ((4, 0, 1), (5, 0, 0), (6, 1, 0)):

            @pl.when(s == turn)
            def _():
                forward(w, kind)

        return carry

    lax.fori_loop(1, max(chain + 3, 7), lat_step, 0)

    for h in range(head_count):
        span = slice(h * head_dim, (h + 1) * head_dim)
        done = (weighted[h] / total[h]).astype(bf16)
        done = done.reshape(teams, part, head_dim)
        for tt in range(teams):
            heads_out[tt % 2, tt // 2, :, span] = done[tt]

    heads_mate = remote(
        heads_out.at[1 - half], heads_in.at[half], core_send.at[1], core_recv.at[1], place(p, mate)
    )
    heads_mate.start()
    heads_in[half] = heads_out[half]
    own_proj.wait()
    for w in range(3):
        w_own(w).wait()
    with jax.named_scope("head_wait"):
        proj_mate.wait_recv()
        heads_mate.wait_recv()

    chunks = share_out.shape[0]
    span_share = share_out.shape[3]

    def project(i, c):
        span = slice(c * span_share, (c + 1) * span_share)
        return jnp.dot(
            heads_in[0, i], proj[0, :, span], preferred_element_type=f32
        ) + jnp.dot(heads_in[1, i], proj[1, :, span], preferred_element_type=f32)

    def share_to(c, step):
        i = lax.rem(column + step, columns)
        return remote(
            share_out.at[c, i],
            share_in.at[c, column],
            share_send.at[c, step],
            share_recv.at[c, step],
            place(p, 2 * i + half),
        )

    with jax.named_scope("project"):
        for c in range(chunks):
            for step in range(1, columns):
                i = lax.rem(column + step, columns)
                share_out[c, i] = project(i, c).astype(bf16)
                share_to(c, step).start()
        forward(1, 1)
        for c in range(chunks):
            span = slice(c * span_share, (c + 1) * span_share)
            wide[:, span] = residual_weight * stream[:, span].astype(f32) + project(column, c)
    for c in range(chunks):
        span = slice(c * span_share, (c + 1) * span_share)
        for step in range(1, columns):
            with jax.named_scope("share_wait"):
                share_to(c, step).wait_recv()
            source = lax.rem(column - step + columns, columns)
            wide[:, span] += share_in[c, source].astype(f32)
    with jax.named_scope("norm"):
        rows[mine] = layer_norm(wide[...], mix_gain[...]).astype(bf16)

    bits = []
    bit = 2
    while bit < teams:
        bits.append(bit)
        bit *= 2
    orders = (bits + [0, 1], [0] + bits + [1])
    depth = len(orders[0])
    sub = part // 2

    def flip(stage, zz, tt):
        if stage == 0:
            return 1 - zz, tt
        return zz, jnp.where((tt // stage) % 2 == 0, tt + stage, tt - stage)

    holdings = []
    for order in orders:
        held = [(layer, t)]
        for stage in order:
            held = held + [flip(stage, zz, tt) for zz, tt in held]
        holdings.append(held)

    def row_copy(o, i, u):
        zz, tt = holdings[o][u]
        index = (tt % 2) * teams + (tt // 2) * 2 + zz
        spot = rows.at[index, pl.ds(o * sub, sub)]
        slot = 2**i - 1 + u
        partner = pair_place(*flip(orders[o][i], layer, t))
        return remote(spot, spot, row_send.at[o, slot], row_recv.at[o, slot], partner)

    for i in range(depth):
        for o in range(2):
            row_copy(o, i, 0).start()
    forward(0, 2)
    forward(1, 2)
    w_own_y(2).start()
    forward(2, 1)
    def row_stage(i):
        for o in range(2):
            for u in range(2**i):
                with jax.named_scope("row_wait"):
                    row_copy(o, i, u).wait_recv()
                for later in range(i + 1, depth):
                    row_copy(o, later, 2**i + u).start()

    def feed(k, carry):
        here = rows[pl.ds(2 * k, 2)].reshape(2 * part, rows.shape[2])
        gate_sum = jnp.dot(
            here, gate[...].reshape(-1, hidden_half), preferred_element_type=f32
        )
        up_sum = jnp.dot(here, up[...].reshape(-1, hidden_half), preferred_element_type=f32)
        value = gate_sum / (1.0 + jnp.exp(-gate_sum)) * up_sum
        hidden[pl.ds(2 * k, 2)] = value.astype(bf16).reshape(2, part, hidden_half)
        return carry

    for i in range(depth - 1):
        row_stage(i)
        if i == 0:
            toward(2, False, start)
    for w in range(2):
        for j in range(chain):
            w_wait(w, j, other)
    with jax.named_scope("feed"):
        lax.fori_loop(half * columns, half * columns + columns, feed, 0)
    forward(2, 2)
    row_stage(depth - 1)
    with jax.named_scope("feed"):
        lax.fori_loop((1 - half) * columns, (1 - half) * columns + columns, feed, 0)

    def block_at(n):
        pair = lax.rem(q // 2 + n // 2, chain // 2)
        inner = 1 - pair % 2
        first = jnp.where(n < 2, layer, inner)
        return 2 * pair + jnp.where(n % 2 == 0, first, 1 - first)

    def term_mate(j):
        return remote(
            terms_out.at[j], mate_in.at[j], mate_send.at[j], mate_recv.at[j], place(p, mate)
        )

    def term_x(j, step):
        i = lax.rem(column + step, columns)
        return remote(
            terms.at[j, i, :, pl.ds(0, sub)],
            x_first.at[j, column],
            term_send.at[j, 0, step],
            term_recv.at[j, 0, step],
            place(p, 2 * i + half),
        )

    def term_z(j):
        return remote(
            terms.at[j, :, 1 - layer, pl.ds(sub, sub)],
            z_first.at[j],
            term_send.at[j, 1, 0],
            term_recv.at[j, 1, 0],
            pair_place(1 - layer, t),
        )

    def relay_x(j, step):
        i = lax.rem(column + step, columns)
        return remote(
            x_relay.at[j, i],
            x_last.at[j, column],
            term_send.at[j, 1, step],
            term_recv.at[j, 1, step],
            place(p, 2 * i + half),
        )

    def relay_z(j):
        return remote(
            z_relay.at[j],
            z_last.at[j],
            term_send.at[j, 0, 0],
            term_recv.at[j, 0, 0],
            pair_place(1 - layer, t),
        )

    def lower(j):
        weights = jnp.concatenate([down[j, 0], down[j, 1]], axis=1)
        own_rows = half * teams

        def product(first):
            here = hidden[pl.ds(first, teams)].reshape(teams * part, hidden_half)
            out = jnp.dot(here, weights, preferred_element_type=f32)
            return out.reshape(columns, 2, part, out.shape[1])

        terms_out[j] = product(teams - own_rows).astype(bf16)
        term_mate(j).start()
        kept = product(own_rows)
        with jax.named_scope("mate_wait"):
            term_mate(j).wait_recv()
        terms[j] = (kept + mate_in[j].astype(f32)).astype(bf16)
        for step in range(1, columns):
            term_x(j, step).start()
        term_z(j).start()

    def sources():
        return [lax.rem(column - step + columns, columns) for step in range(1, columns)]

    def relay(j):
        with jax.named_scope("relay_wait"):
            for step in range(1, columns):
                term_x(j, step).wait_recv()
            term_z(j).wait_recv()
        far = terms[j, column, 1 - layer, :sub].astype(f32)
        for source in sources():
            far = far + x_first[j, source, 1 - layer].astype(f32)
        z_relay[j] = far.astype(bf16)
        relay_z(j).start()
        for step in range(1, columns):
            i = lax.rem(column + step, columns)
            side = terms[j, i, layer, sub:].astype(f32) + z_first[j, i].astype(f32)
            x_relay[j, i] = side.astype(bf16)
            relay_x(j, step).start()

    def lower_step(n, carry):
        j = block_at(n)
        w_wait(2, j, other)
        with jax.named_scope("lower"):
            lower(j)

        @pl.when(n == 1)
        def _():
            forward(2, 0)

        @pl.when(n > 0)
        def _():
            relay(block_at(n - 1))

        return carry

    lax.fori_loop(0, chain, lower_step, 0)
    relay(block_at(chain - 1))
    span_width = terms.shape[4]
    for j in range(chain):
        with jax.named_scope("term_wait"):
            relay_z(j).wait_recv()
            for step in range(1, columns):
                relay_x(j, step).wait_recv()
        span = slice(j * span_width, (j + 1) * span_width)
        top_rows = terms[j, column, layer, :sub].astype(f32) + z_last[j].astype(f32)
        low_rows = terms[j, column, layer, sub:].astype(f32) + z_first[j, column].astype(f32)
        for source in sources():
            top_rows = top_rows + x_first[j, source, layer].astype(f32)
            low_rows = low_rows + x_last[j, source].astype(f32)
        kept_rows = residual_weight * rows[mine, :, span].astype(f32)
        wide[:sub, span] = kept_rows[:sub] + 0.5 * top_rows
        wide[sub:, span] = kept_rows[sub:] + 0.5 * low_rows
    with jax.named_scope("norm"):
        result[...] = layer_norm(wide[...], mlp_gain[...]).astype(bf16)

    proj_mate.wait_send()
    heads_mate.wait_send()
    for c in range(chunks):
        for step in range(1, columns):
            share_to(c, step).wait_send()
    for o in range(2):
        for i in range(depth):
            for u in range(2**i):
                row_copy(o, i, u).wait_send()

    @pl.when(p == 0)
    def _():
        lat_own_y().wait_send()

    for w in range(3):
        w_own_y(w).wait_send()

    def drain(j, carry):
        term_mate(j).wait_send()
        term_z(j).wait_send()
        relay_z(j).wait_send()
        for step in range(1, columns):
            term_x(j, step).wait_send()
            relay_x(j, step).wait_send()

        @pl.when(j != q)
        def _():
            for w in range(3):
                w_to_y(w, j).wait_send()

        @pl.when(j < q)
        def _():
            lat_to_y(j).wait_send()

            @pl.when(layer == 0)
            def _():
                lat_to_next(j).wait_send()

            for step in far_steps:
                lat_to_x(j, p, step).wait_send()

                @pl.when(turned(j))
                def _():
                    lat_side(j, step).wait_send()

            for i in range(columns):
                lat_to_m(j, p, 2 * i + half).wait_send()

        @pl.when((j < q) | ((j == q) & (p == 1)))
        def _():
            @pl.when(jnp.logical_not(turned(j)))
            def _():
                for step in far_steps:
                    lat_to_x(j, other, step).wait_send()

            for i in range(columns):
                lat_to_m(j, other, 2 * i + half).wait_send()

        return carry

    lax.fori_loop(0, chain, drain, 0)
    lat_own_to_z(sent)
    for w in range(3):
        toward(w, False, sent)
        toward(w, True, sent)
        away(w, sent)


def per_device(
    chain,
    teams,
    queries_nope,
    queries_rope,
    latent,
    rope_key,
    latent_gain,
    key_up,
    value_up,
    out_proj,
    stream,
    mix_gain,
    w_gate,
    w_up,
    w_down,
    mlp_gain,
):
    row_count, head_count, head_dim = queries_nope.shape
    rope_dim = queries_rope.shape[2]
    first_row = lax.axis_index("sp") * row_count
    query_turned = rotate(queries_rope.astype(jnp.float32), first_row).astype(jnp.bfloat16)
    key_turned = rotate(rope_key.astype(jnp.float32), first_row).astype(jnp.bfloat16)
    normed = latent_norm(latent, latent_gain)
    scale = (head_dim + rope_dim) ** (-0.5) * math.log2(math.e)
    spare = -rope_dim % 128
    qcat = jnp.concatenate(
        [queries_nope, query_turned, jnp.zeros((row_count, head_count, spare), bf16)], axis=2
    ).transpose(1, 0, 2)
    latent_in = jnp.concatenate(
        [normed, key_turned, jnp.zeros((row_count, spare), bf16)], axis=1
    ).reshape(teams, row_count // teams, -1)
    width = latent_in.shape[2]
    model, hidden_here = w_gate.shape[0] * 2 * chain, w_gate.shape[1]
    group = 2 * teams
    part = row_count // teams
    half_hidden = hidden_here // 2
    deep = w_gate.shape[0]
    slim = w_down.shape[1]
    stages = group - 1
    chunks = 4
    dma = pltpu.SemaphoreType.DMA
    vmem = pl.BlockSpec(memory_space=pltpu.VMEM)
    hbm = pl.BlockSpec(memory_space=pltpu.HBM)
    return pl.pallas_call(
        functools.partial(layer_kernel, chain, teams, scale),
        out_shape=jax.ShapeDtypeStruct((part, model), bf16),
        in_specs=[vmem, hbm, vmem, vmem, hbm, vmem, vmem, hbm, hbm, hbm, vmem],
        out_specs=vmem,
        scratch_shapes=[
            pltpu.VMEM((chain, 2, teams, part, width), bf16),
            pltpu.VMEM((chain, 2, deep, half_hidden), bf16),
            pltpu.VMEM((chain, 2, deep, half_hidden), bf16),
            pltpu.VMEM((chain, 2, half_hidden, slim), bf16),
            pltpu.VMEM((2,) + out_proj.shape, bf16),
            pltpu.VMEM((2, teams // 2, part, head_count * head_dim), bf16),
            pltpu.VMEM((2, teams // 2, part, head_count * head_dim), bf16),
            pltpu.VMEM((chunks, teams // 2, part, model // chunks), bf16),
            pltpu.VMEM((chunks, teams // 2, part, model // chunks), bf16),
            pltpu.VMEM((group, part, model), bf16),
            pltpu.VMEM((group, part, half_hidden), bf16),
            pltpu.VMEM((chain, teams // 2, 2, part, 2 * slim), bf16),
            pltpu.VMEM((chain, teams // 2, 2, part, 2 * slim), bf16),
            pltpu.VMEM((chain, teams // 2, 2, part, 2 * slim), bf16),
            pltpu.VMEM((chain, teams // 2, 2, part // 2, 2 * slim), bf16),
            pltpu.VMEM((chain, teams // 2, part // 2, 2 * slim), bf16),
            pltpu.VMEM((chain, teams // 2, part // 2, 2 * slim), bf16),
            pltpu.VMEM((chain, part // 2, 2 * slim), bf16),
            pltpu.VMEM((chain, teams // 2, part // 2, 2 * slim), bf16),
            pltpu.VMEM((chain, part // 2, 2 * slim), bf16),
            pltpu.VMEM((part, model), f32),
            pltpu.VMEM((head_count, row_count, 1), f32),
            pltpu.VMEM((head_count, row_count, 1), f32),
            pltpu.VMEM((head_count, row_count, head_dim), f32),
            dma((5,)),
            dma((chain, 2, teams)),
            dma((chain,)),
            dma((chain,)),
            dma((chain, teams)),
            dma((chain,)),
            dma((chain, 2, teams)),
            dma((chain, 2, teams)),
            dma((3, chain, 2)),
            dma((3, chain)),
            dma((3, chain)),
            dma((2,)),
            dma((2,)),
            dma((chunks, teams)),
            dma((chunks, teams)),
            dma((2, stages)),
            dma((2, stages)),
            dma((chain,)),
            dma((chain,)),
            dma((chain, 2, teams)),
            dma((chain, 2, teams)),
        ],
        compiler_params=pltpu.CompilerParams(
            collective_id=0, has_side_effects=True, vmem_limit_bytes=60 * 1024 * 1024
        ),
    )(
        qcat,
        latent_in,
        key_up,
        value_up,
        out_proj,
        stream,
        mix_gain.reshape(1, -1),
        w_gate,
        w_up,
        w_down,
        mlp_gain.reshape(1, -1),
    )


def solution(mesh):
    return jax.shard_map(
        functools.partial(per_device, mesh.shape["sp"] // 2, mesh.shape["tp"]),
        mesh=mesh,
        in_specs=(
            P("sp", "tp", None),
            P("sp", "tp", None),
            P("sp", None),
            P("sp", None),
            P(),
            P(None, "tp"),
            P(None, "tp"),
            P("tp", None),
            P(("sp", "tp"), None),
            P(),
            P("sp", "tp"),
            P("sp", "tp"),
            P("tp", "sp"),
            P(),
        ),
        out_specs=P(("sp", "tp"), None),
        check_vma=False,
    )
```

```python
import functools
import math

import jax
import jax.numpy as jnp
import numpy as np
from jax import lax
from jax.experimental import pallas as pl
from jax.experimental.pallas import tpu as pltpu
from jax.sharding import PartitionSpec as P

theta_base = 10000.0
residual_weight = 8.0**0.25
norm_floor = 1.0
big_negative = -1e30


def latent_norm(latent, latent_gain):
    wide = latent.astype(jnp.float32)
    factor = lax.rsqrt(jnp.mean(wide * wide, axis=-1, keepdims=True) + norm_floor)
    return (wide * factor * latent_gain).astype(jnp.bfloat16)


def layer_norm(values, gain):
    centre = jnp.mean(values, axis=-1, keepdims=True)
    centred = values - centre
    spread = jnp.mean(centred * centred, axis=-1, keepdims=True)
    return centred * lax.rsqrt(spread + norm_floor) * gain


mesh_id = pl.DeviceIdType.MESH
bf16 = jnp.bfloat16
f32 = jnp.float32


def layer_kernel(
    chain,
    teams,
    scale,
    rope_dim,
    nope_hbm,
    rope_hbm,
    latent_hbm,
    rope_key_hbm,
    latent_gain_hbm,
    rates_hbm,
    key_up_hbm,
    value_up_hbm,
    proj_in,
    stream_hbm,
    mix_gain_hbm,
    gate_in,
    up_in,
    down_in,
    mlp_gain_hbm,
    result,
    nope,
    rope,
    latent_in,
    rope_key,
    latent_gain,
    rates,
    key_up,
    value_up,
    stream,
    mix_gain,
    mlp_gain,
    qcat,
    lat,
    gate,
    up,
    down,
    proj,
    heads_out,
    heads_in,
    share_out,
    share_in,
    rows,
    hidden,
    terms_out,
    mate_in,
    terms,
    x_first,
    z_first,
    x_relay,
    z_relay,
    x_last,
    z_last,
    wide,
    top,
    total,
    weighted,
    load_sem,
    local_sem,
    lat_recv,
    lat_z,
    lat_y,
    lat_w,
    lat_next,
    lat_x,
    lat_m,
    w_recv,
    w_z,
    w_y,
    core_recv,
    core_send,
    share_recv,
    share_send,
    row_recv,
    row_send,
    mate_recv,
    mate_send,
    term_recv,
    term_send,
):
    sp = lax.axis_index("sp")
    t = lax.axis_index("tp")
    q = sp // 2
    p = sp % 2
    other = 1 - p
    half = t % 2
    column = t // 2
    columns = teams // 2
    mate = t + 1 - 2 * half
    layer = q % 2
    group = 2 * teams
    mine = half * teams + column * 2 + layer
    last = chain - 1
    head_count = qcat.shape[0]
    head_dim = value_up.shape[1] // head_count
    block_rows = qcat.shape[1]
    width = value_up.shape[0]
    part = block_rows // teams

    def place(pp, tt, qq=None):
        return ((q if qq is None else qq) * 2 + pp, tt)

    def across(step):
        return lax.rem(t + step, teams)

    def remote(source, target, send, recv, device):
        return pltpu.make_async_remote_copy(
            src_ref=source,
            dst_ref=target,
            send_sem=send,
            recv_sem=recv,
            device_id=device,
            device_id_type=mesh_id,
        )

    def pair_place(zz, tt):
        return place(p, tt, q - layer + zz)

    far_steps = range(2, teams, 2)
    barrier = pltpu.get_barrier_semaphore()
    peers = [place(p, t, lax.rem(q + d, chain)) for d in range(1, chain)]
    peers += [place(other, t), place(p, mate)]
    peers += [place(p, across(step)) for step in far_steps]
    peers += [pair_place(1 - layer, across(step)) for step in far_steps]
    for device in peers:
        pl.semaphore_signal(barrier, inc=1, device_id=device, device_id_type=mesh_id)

    loads = [
        pltpu.make_async_copy(source, target, load_sem.at[i])
        for i, (source, target) in enumerate(
            (
                (latent_hbm, latent_in),
                (rope_key_hbm, rope_key),
                (latent_gain_hbm, latent_gain),
                (rates_hbm, rates),
                (rope_hbm, rope),
                (nope_hbm, nope),
                (key_up_hbm, key_up),
                (value_up_hbm, value_up),
                (stream_hbm, stream),
                (mix_gain_hbm, mix_gain),
                (mlp_gain_hbm, mlp_gain),
            )
        )
    ]
    for load in loads:
        load.start()

    def lat_to_z(qq):
        return remote(
            lat.at[q, p, t], lat.at[q, p, t], lat_z.at[qq], lat_recv.at[q, p, t], place(p, t, qq)
        )

    def lat_to_next(j):
        spot = lat.at[j, p, t]
        return remote(spot, spot, lat_next.at[j], lat_recv.at[j, p, t], place(p, t, q + 1))

    def lat_side(j, step):
        spot = lat.at[j, p, across(step)]
        return remote(
            spot, spot, lat_w.at[j, step // 2 - 1], lat_recv.at[j, p, across(step)], place(other, t)
        )

    def turned(j):
        return (j % 2 == 1) & (j < q)

    def lat_own_y():
        return remote(
            lat.at[q, p, t], lat.at[q, p, t], lat_y.at[q], lat_recv.at[q, p, t], place(other, t)
        )

    def lat_to_y(j):
        spot = lat.at[j, p, t]
        return remote(spot, spot, lat_y.at[j], lat_recv.at[j, p, t], place(other, t))

    def lat_to_x(j, pp, step):
        spot = lat.at[j, pp, t]
        return remote(
            spot, spot, lat_x.at[j, pp, step // 2 - 1], lat_recv.at[j, pp, t], place(p, across(step))
        )

    def lat_to_m(j, pp, tt):
        spot = lat.at[j, pp, tt]
        return remote(spot, spot, lat_m.at[j, pp, tt // 2], lat_recv.at[j, pp, tt], place(p, mate))

    def lat_wait(j, pp, tt):
        spot = lat.at[j, pp, tt]
        with jax.named_scope("lat_wait"):
            remote(spot, spot, lat_y.at[0], lat_recv.at[j, pp, tt], place(p, mate)).wait_recv()

    stores = (gate, up, down)
    hidden_half = gate.shape[3]

    def piece(w, which):
        start = pl.multiple_of(which * hidden_half, 128)
        if w == 0:
            return gate_in.at[:, pl.ds(start, hidden_half)]
        if w == 1:
            return up_in.at[:, pl.ds(start, hidden_half)]
        return down_in.at[pl.ds(start, hidden_half), :]

    def w_to_z(w, qq):
        return remote(
            piece(w, qq % 2),
            stores[w].at[q, p],
            w_z.at[w, qq],
            w_recv.at[w, q, p],
            place(p, t, qq),
        )

    def w_own_y(w):
        return remote(
            piece(w, layer), stores[w].at[q, p], w_y.at[w, q], w_recv.at[w, q, p], place(other, t)
        )

    def w_to_y(w, j):
        spot = stores[w].at[j, p]
        return remote(spot, spot, w_y.at[w, j], w_recv.at[w, j, p], place(other, t))

    def w_wait(w, j, pp):
        spot = stores[w].at[j, pp]
        with jax.named_scope("w_wait"):
            remote(spot, spot, w_y.at[w, 0], w_recv.at[w, j, pp], place(p, mate)).wait_recv()

    def w_own(w):
        return pltpu.make_async_copy(piece(w, layer), stores[w].at[q, p], local_sem.at[1 + w])

    own_proj = pltpu.make_async_copy(proj_in, proj.at[half], local_sem.at[4])
    proj_mate = remote(proj_in, proj.at[half], core_send.at[0], core_recv.at[0], place(p, mate))

    beyond = range(2, chain)

    def lat_own_to_z(act):
        for d in range(1, chain):

            takes = (q + d <= last) & (((q + d) % 2 == 0) | ((d == 1) & (layer == 0)))

            @pl.when(takes)
            def _():
                act(lat_to_z(q + d))

    def toward(w, near, act):
        for d in (1,) if near else range(2, chain) if w == 2 else range(last, 1, -1):

            @pl.when((layer == 0) & (q + d <= last))
            def _():
                act(w_to_z(w, q + d))

            @pl.when((layer == 1) & (q - d >= 0))
            def _():
                act(w_to_z(w, q - d))

    def away(w, distances, act):
        for d in distances:

            @pl.when((layer == 1) & (q + d <= last))
            def _():
                act(w_to_z(w, q + d))

            @pl.when((layer == 0) & (q - d >= 0))
            def _():
                act(w_to_z(w, q - d))

    def start(copy):
        copy.start()

    def sent(copy):
        copy.wait_send()

    for w in range(3):
        w_own(w).start()
    own_proj.start()

    lanes = head_count * rope_dim
    turn_rows = lax.broadcasted_iota(jnp.int32, (block_rows, lanes), 0)
    turn_lanes = lax.broadcasted_iota(jnp.int32, (block_rows, lanes), 1)
    left = lax.rem(turn_lanes, rope_dim) < rope_dim // 2
    loads[3].wait()
    with jax.named_scope("angles"):
        angle = (sp * block_rows + turn_rows).astype(f32) * rates[...]
        cosine = jnp.cos(angle)
        sine = jnp.sin(angle)
        sine = jnp.where(left, -sine, sine)

    def turn(vector):
        ahead = pltpu.roll(vector, lanes - rope_dim // 2, 1)
        behind = pltpu.roll(vector, rope_dim // 2, 1)
        return vector * cosine + jnp.where(left, ahead, behind) * sine

    def alone(vector):
        return jnp.where(turn_lanes < rope_dim, vector, 0.0).astype(bf16)

    for load in loads[:3]:
        load.wait()
    with jax.named_scope("latent"):
        lat[q, p, :, :, :width] = latent_norm(latent_in[...], latent_gain[...]).reshape(
            teams, part, width
        )
        key = rope_key[...].astype(f32)
        key = turn(jnp.concatenate([key] * head_count, axis=0).T)
        lat[q, p, :, :, width:] = alone(key).reshape(teams, part, lanes)
    with jax.named_scope("barrier"):
        pl.semaphore_wait(barrier, len(peers))
    lat_own_to_z(start)

    @pl.when(p == 0)
    def _():
        lat_own_y().start()

    w_own_y(0).start()
    patient = q == last - 1

    def all_toward():
        toward(0, True, start)

        @pl.when(layer == 0)
        def _():
            toward(1, True, start)

            @pl.when(jnp.logical_not(patient))
            def _():
                toward(2, True, start)

        toward(0, False, start)
        toward(1, False, start)

        @pl.when(layer == 1)
        def _():
            toward(1, True, start)
            toward(2, True, start)

    for w, distances in ((0, (1,)), (1, (1,)), (0, beyond), (1, beyond), (2, (1,))):
        away(w, distances, start)

    @pl.when(jnp.logical_not(patient))
    def _():
        all_toward()

    proj_mate.start()
    for load in loads[4:6]:
        load.wait()
    turned_queries = turn(rope[...].astype(f32).T)
    for h in range(head_count):
        qcat[h, :, :head_dim] = nope[:, h * head_dim : (h + 1) * head_dim]
        shifted = turned_queries if h == 0 else pltpu.roll(turned_queries, lanes - h * rope_dim, 1)
        qcat[h, :, head_dim:] = alone(shifted)

    top[...] = jnp.full_like(top, big_negative)
    total[...] = jnp.zeros_like(total)
    weighted[...] = jnp.zeros_like(weighted)

    def attend(j, pp, diagonal):
        block = lat[j, pp].reshape(block_rows, lat.shape[4])
        normed = block[:, :width]
        rotary = block[:, width:]
        keys = jnp.dot(normed, key_up[...], preferred_element_type=f32).astype(bf16)
        values = jnp.dot(normed, value_up[...], preferred_element_type=f32).astype(bf16)
        for h in range(head_count):
            span = slice(h * head_dim, (h + 1) * head_dim)
            both = jnp.concatenate([keys[:, span], rotary], axis=1)
            score = lax.dot_general(
                qcat[h], both, (((1,), (1,)), ((), ())), preferred_element_type=f32
            )
            if diagonal:
                down_rows = lax.broadcasted_iota(jnp.int32, score.shape, 0)
                over_columns = lax.broadcasted_iota(jnp.int32, score.shape, 1)
                score = jnp.where(over_columns <= down_rows, score, big_negative)
            old = top[h]
            new = jnp.maximum(old, jnp.max(score, axis=1, keepdims=True))
            powers = jnp.exp2(score * scale - new * scale)
            shrink = jnp.exp2((old - new) * scale)
            total[h] = total[h] * shrink + jnp.sum(powers, axis=1, keepdims=True)
            weighted[h] = weighted[h] * shrink + jnp.dot(
                powers.astype(bf16), values[:, span], preferred_element_type=f32
            )
            top[h] = new

    for load in loads[6:]:
        load.wait()
    with jax.named_scope("attend_own"):
        attend(q, p, True)

    own = "own"

    def is_edge(j):
        return (j % 4 == 0) | (j % 4 == 3)

    def forward(w, kind):
        for j in range(chain):
            distant = q // 2 != j // 2
            if kind == 1:
                takes = (q // 2 == j // 2) & (q != j)
            elif is_edge(j) == (kind == 0):
                takes = distant
            else:
                continue

            @pl.when(takes)
            def _():
                w_wait(w, j, p)
                w_to_y(w, j).start()

    plans = {
        "early": (((0, 1),), ((0, 2), (0, 1)), ((0, 1),), ()),
        "late": (((0, 0), (1, 1)), ((0, 0), (1, 1)), ((0, 2),), (own,)),
        "after": ((), (), ((1, 2), own), ((0, 0),)),
        "share": (((1, 0), own, (2, 1)), ((1, 0),), ((1, 1),), ((0, 1),)),
        "half": ((), (), (), ((1, 0), (1, 1))),
        "rows": ((), ((1, 2), own, (2, 1)), ((0, 0), (1, 0)), ((0, 2), (1, 2))),
        "near": (((0, 2),), (), ((2, 1),), ()),
        "middle": (((1, 2),), (), (), ()),
        "far": ((), (), ((2, 2),), ()),
        "last": (((2, 2),), ((2, 2),), ((2, 0),), ((2, 0),)),
        "end": ((), ((2, 0),), (), ((2, 2),)),
        "loop": (((2, 0),), (), (), ((2, 1),)),
    }

    def pass_along(name):
        for kind_of, plan in enumerate(plans[name]):
            if plan:

                @pl.when(q % 4 == kind_of)
                def _():
                    for entry in plan:
                        if entry is own:
                            w_own_y(2).start()
                        else:
                            forward(*entry)

    def lat_step(s, carry):
        a = q - s

        @pl.when(a >= 0)
        def _():
            lat_wait(a, p, t)
            lat_to_y(a).start()
            for step in far_steps:
                lat_to_x(a, p, step).start()
            lat_to_m(a, p, t).start()

            @pl.when(layer == 0)
            def _():
                lat_to_next(a).start()

        b = q - s + 1

        @pl.when((b >= 0) & ((s >= 2) | (p == 1)))
        def _():
            lat_wait(b, other, t)

            @pl.when(jnp.logical_not(turned(b)))
            def _():
                for step in far_steps:
                    lat_to_x(b, other, step).start()

            lat_to_m(b, other, t).start()

        @pl.when(s == 3)
        def _():
            w_own_y(1).start()

        @pl.when((s == 3) & patient)
        def _():
            all_toward()

        def block(j, pp):
            for i in range(columns):
                lat_wait(j, pp, 2 * i + 1 - half)
            with jax.named_scope("attend"):
                attend(j, pp, False)

        def stage(k, inner):
            e = q - s + 2 + k

            @pl.when((e >= 0) & ((s >= 4) | ((s == 3) & ((k == 0) | (p == 1)))))
            def _():
                block(e, jnp.where(k == 0, p, other))

            c = b + k
            side = jnp.where(k == 0, p, other)
            ready = (s >= 2) & ((k == 0) | (s >= 3) | (p == 1))

            @pl.when((c >= 0) & ready)
            def _():
                for step in far_steps:
                    lat_wait(c, side, across(step))

                    @pl.when(turned(c) & (k == 0))
                    def _():
                        lat_side(c, step).start()

                    lat_to_m(c, side, across(step)).start()

            return inner

        lax.fori_loop(0, 2, stage, 0)
        for turn, name in ((4, "early"), (5, "late")):

            @pl.when(s == turn)
            def _():
                pass_along(name)

        return carry

    lax.fori_loop(1, max(chain + 3, 6), lat_step, 0)
    pass_along("after")


    for h in range(head_count):
        span = slice(h * head_dim, (h + 1) * head_dim)
        done = (weighted[h] / total[h]).astype(bf16)
        done = done.reshape(teams, part, head_dim)
        for tt in range(teams):
            heads_out[tt % 2, tt // 2, :, span] = done[tt]

    heads_mate = remote(
        heads_out.at[1 - half], heads_in.at[half], core_send.at[1], core_recv.at[1], place(p, mate)
    )
    heads_mate.start()
    heads_in[half] = heads_out[half]
    own_proj.wait()
    for w in range(3):
        w_own(w).wait()
    with jax.named_scope("head_wait"):
        proj_mate.wait_recv()
        heads_mate.wait_recv()

    chunks = share_out.shape[0]
    span_share = share_out.shape[3]

    def project(i, c):
        span = slice(c * span_share, (c + 1) * span_share)
        return jnp.dot(
            heads_in[0, i], proj[0, :, span], preferred_element_type=f32
        ) + jnp.dot(heads_in[1, i], proj[1, :, span], preferred_element_type=f32)

    def share_to(c, step):
        i = lax.rem(column + step, columns)
        return remote(
            share_out.at[c, i],
            share_in.at[c, column],
            share_send.at[c, step - 1],
            share_recv.at[c, step - 1],
            place(p, 2 * i + half),
        )

    with jax.named_scope("project"):
        for c in range(chunks):
            for step in range(1, columns):
                i = lax.rem(column + step, columns)
                share_out[c, i] = project(i, c).astype(bf16)
                share_to(c, step).start()
        pass_along("share")
        for c in range(chunks):
            span = slice(c * span_share, (c + 1) * span_share)
            wide[:, span] = residual_weight * stream[:, span].astype(f32) + project(column, c)
    for c in range(chunks):
        span = slice(c * span_share, (c + 1) * span_share)
        for step in range(1, columns):
            with jax.named_scope("share_wait"):
                share_to(c, step).wait_recv()
            source = lax.rem(column - step + columns, columns)
            wide[:, span] += share_in[c, source].astype(f32)
        if c == 1:
            pass_along("half")
    with jax.named_scope("norm"):
        rows[mine] = layer_norm(wide[...], mix_gain[...]).astype(bf16)

    bits = []
    bit = 2
    while bit < teams:
        bits.append(bit)
        bit *= 2
    orders = (bits + [0, 1], [0] + bits + [1])
    depth = len(orders[0])
    sub = part // 2

    def flip(stage, zz, tt):
        if stage == 0:
            return 1 - zz, tt
        return zz, jnp.where((tt // stage) % 2 == 0, tt + stage, tt - stage)

    holdings = []
    for order in orders:
        held = [(layer, t)]
        for stage in order:
            held = held + [flip(stage, zz, tt) for zz, tt in held]
        holdings.append(held)

    def row_copy(o, i, u):
        zz, tt = holdings[o][u]
        index = (tt % 2) * teams + (tt // 2) * 2 + zz
        spot = rows.at[index, pl.ds(o * sub, sub)]
        slot = 2**i - 1 + u
        partner = pair_place(*flip(orders[o][i], layer, t))
        return remote(spot, spot, row_send.at[o, slot], row_recv.at[o, slot], partner)

    for i in range(depth):
        for o in range(2):
            row_copy(o, i, 0).start()
    pass_along("rows")
    def row_stage(i):
        for o in range(2):
            for u in range(2**i):
                with jax.named_scope("row_wait"):
                    row_copy(o, i, u).wait_recv()
                for later in range(i + 1, depth):
                    row_copy(o, later, 2**i + u).start()

    def feed(k, carry):
        here = rows[pl.ds(2 * k, 2)].reshape(2 * part, rows.shape[2])
        gate_sum = jnp.dot(
            here, gate[...].reshape(-1, hidden_half), preferred_element_type=f32
        )
        up_sum = jnp.dot(here, up[...].reshape(-1, hidden_half), preferred_element_type=f32)
        value = gate_sum / (1.0 + jnp.exp(-gate_sum)) * up_sum
        hidden[pl.ds(2 * k, 2)] = value.astype(bf16).reshape(2, part, hidden_half)
        return carry

    for i in range(depth - 1):
        row_stage(i)
        if i == 0:
            pass_along("near")

            toward(2, False, start)

            @pl.when(patient)
            def _():
                toward(2, True, start)

            @pl.when(layer == 0)
            def _():
                away(2, beyond, start)

            pass_along("middle")

    @pl.when(layer == 1)
    def _():
        away(2, beyond, start)

    pass_along("far")
    for w in range(2):
        for j in range(chain):
            w_wait(w, j, other)
    with jax.named_scope("feed"):
        lax.fori_loop(half * columns, half * columns + columns, feed, 0)
    pass_along("last")
    row_stage(depth - 1)
    with jax.named_scope("feed"):
        lax.fori_loop((1 - half) * columns, (1 - half) * columns + columns, feed, 0)

    def settle(j, carry):
        @pl.when(j != q)
        def _():
            for w in range(2):
                w_to_y(w, j).wait_send()

        @pl.when(j < q)
        def _():
            lat_to_y(j).wait_send()

            @pl.when(layer == 0)
            def _():
                lat_to_next(j).wait_send()

            for step in far_steps:
                lat_to_x(j, p, step).wait_send()

                @pl.when(turned(j))
                def _():
                    lat_side(j, step).wait_send()

            for i in range(columns):
                lat_to_m(j, p, 2 * i + half).wait_send()

        @pl.when((j < q) | ((j == q) & (p == 1)))
        def _():
            @pl.when(jnp.logical_not(turned(j)))
            def _():
                for step in far_steps:
                    lat_to_x(j, other, step).wait_send()

            for i in range(columns):
                lat_to_m(j, other, 2 * i + half).wait_send()

        return carry

    with jax.named_scope("settle"):
        proj_mate.wait_send()
        heads_mate.wait_send()
        for c in range(chunks):
            for step in range(1, columns):
                share_to(c, step).wait_send()

        @pl.when(p == 0)
        def _():
            lat_own_y().wait_send()

        lax.fori_loop(0, chain, settle, 0)
        lat_own_to_z(sent)
        for w in range(2):
            w_own_y(w).wait_send()
            toward(w, False, sent)
            toward(w, True, sent)
            away(w, range(1, chain), sent)
    pass_along("end")

    def block_at(n):
        here = q // 2
        upper = here % 2
        skip = 2 - upper
        ahead = jnp.maximum(n - skip, 0)
        there = lax.rem(here + 1 + ahead // 2, chain // 2)
        edge = 2 * there + there % 2
        distant = jnp.where((ahead + upper) % 2 == 1, edge, 4 * there + 1 - edge)
        own_edge = 2 * here + upper
        own_inner = 4 * here + 1 - own_edge
        chosen = jnp.where(n == 0, own_edge, jnp.where(n < skip, own_inner, distant))
        return jnp.where((upper == 1) & (n == chain - 1), own_inner, chosen)

    def term_mate(j):
        return remote(
            terms_out.at[j], mate_in.at[j], mate_send.at[j], mate_recv.at[j], place(p, mate)
        )

    def term_x(j, step):
        i = lax.rem(column + step, columns)
        return remote(
            terms.at[j, i, :, pl.ds(0, sub)],
            x_first.at[j, column],
            term_send.at[j, 0, step],
            term_recv.at[j, 0, step],
            place(p, 2 * i + half),
        )

    def term_z(j):
        return remote(
            terms.at[j, :, 1 - layer, pl.ds(sub, sub)],
            z_first.at[j],
            term_send.at[j, 1, 0],
            term_recv.at[j, 1, 0],
            pair_place(1 - layer, t),
        )

    def relay_x(j, step):
        i = lax.rem(column + step, columns)
        return remote(
            x_relay.at[j, i],
            x_last.at[j, column],
            term_send.at[j, 1, step],
            term_recv.at[j, 1, step],
            place(p, 2 * i + half),
        )

    def relay_z(j):
        return remote(
            z_relay.at[j],
            z_last.at[j],
            term_send.at[j, 0, 0],
            term_recv.at[j, 0, 0],
            pair_place(1 - layer, t),
        )

    own_rows = half * teams

    def product(j, first):
        weights = jnp.concatenate([down[j, 0], down[j, 1]], axis=1)
        here = hidden[pl.ds(first, teams)].reshape(teams * part, hidden_half)
        out = jnp.dot(here, weights, preferred_element_type=f32)
        return out.reshape(columns, 2, part, out.shape[1])

    def lower_mate(j):
        terms_out[j] = product(j, teams - own_rows).astype(bf16)
        term_mate(j).start()

    def lower_own(j):
        kept = product(j, own_rows)
        with jax.named_scope("mate_wait"):
            term_mate(j).wait_recv()
        terms[j] = (kept + mate_in[j].astype(f32)).astype(bf16)
        for step in range(1, columns):
            term_x(j, step).start()
        term_z(j).start()

    def sources():
        return [lax.rem(column - step + columns, columns) for step in range(1, columns)]

    def relay(j):
        with jax.named_scope("relay_wait"):
            for step in range(1, columns):
                term_x(j, step).wait_recv()
            term_z(j).wait_recv()
        far = terms[j, column, 1 - layer, :sub].astype(f32)
        for source in sources():
            far = far + x_first[j, source, 1 - layer].astype(f32)
        z_relay[j] = far.astype(bf16)
        relay_z(j).start()
        for step in range(1, columns):
            i = lax.rem(column + step, columns)
            side = terms[j, i, layer, sub:].astype(f32) + z_first[j, i].astype(f32)
            x_relay[j, i] = side.astype(bf16)
            relay_x(j, step).start()

    def lower_step(n, carry):
        @pl.when(n < chain)
        def _():
            j = block_at(n)
            w_wait(2, j, other)
            with jax.named_scope("lower_mate"):
                lower_mate(j)

        @pl.when((n >= 1) & (n <= chain))
        def _():
            with jax.named_scope("lower_own"):
                lower_own(block_at(n - 1))

        @pl.when(n == 1)
        def _():
            pass_along("loop")

        @pl.when(n >= 3)
        def _():
            relay(block_at(n - 3))

        return carry

    lax.fori_loop(0, chain + 3, lower_step, 0)
    span_width = terms.shape[4]
    for j in range(chain):
        with jax.named_scope("term_wait"):
            relay_z(j).wait_recv()
            for step in range(1, columns):
                relay_x(j, step).wait_recv()
        span = slice(j * span_width, (j + 1) * span_width)
        top_rows = terms[j, column, layer, :sub].astype(f32) + z_last[j].astype(f32)
        low_rows = terms[j, column, layer, sub:].astype(f32) + z_first[j, column].astype(f32)
        for source in sources():
            top_rows = top_rows + x_first[j, source, layer].astype(f32)
            low_rows = low_rows + x_last[j, source].astype(f32)
        kept_rows = residual_weight * rows[mine, :, span].astype(f32)
        wide[:sub, span] = kept_rows[:sub] + 0.5 * top_rows
        wide[sub:, span] = kept_rows[sub:] + 0.5 * low_rows
    with jax.named_scope("norm"):
        result[...] = layer_norm(wide[...], mlp_gain[...]).astype(bf16)

    for o in range(2):
        for i in range(depth):
            for u in range(2**i):
                row_copy(o, i, u).wait_send()
    w_own_y(2).wait_send()
    toward(2, False, sent)
    toward(2, True, sent)
    away(2, range(1, chain), sent)

    def drain(j, carry):
        term_mate(j).wait_send()
        term_z(j).wait_send()
        relay_z(j).wait_send()
        for step in range(1, columns):
            term_x(j, step).wait_send()
            relay_x(j, step).wait_send()

        @pl.when(j != q)
        def _():
            w_to_y(2, j).wait_send()

        return carry

    with jax.named_scope("drain"):
        lax.fori_loop(0, chain, drain, 0)


def per_device(
    chain,
    teams,
    queries_nope,
    queries_rope,
    latent,
    rope_key,
    latent_gain,
    key_up,
    value_up,
    out_proj,
    stream,
    mix_gain,
    w_gate,
    w_up,
    w_down,
    mlp_gain,
):
    row_count, head_count, head_dim = queries_nope.shape
    rope_dim = queries_rope.shape[2]
    scale = (head_dim + rope_dim) ** (-0.5) * math.log2(math.e)
    lanes = head_count * rope_dim
    half_rope = rope_dim // 2
    rates = theta_base ** (-2.0 * (np.arange(lanes) % half_rope) / rope_dim)
    rates = jnp.asarray(rates, f32).reshape(1, lanes)
    rank = latent.shape[1]
    width = rank + lanes
    model, hidden_here = w_gate.shape[0] * 2 * chain, w_gate.shape[1]
    group = 2 * teams
    part = row_count // teams
    half_hidden = hidden_here // 2
    deep = w_gate.shape[0]
    slim = w_down.shape[1]
    stages = group - 1
    chunks = 4
    dma = pltpu.SemaphoreType.DMA
    vmem = pl.BlockSpec(memory_space=pltpu.VMEM)
    hbm = pl.BlockSpec(memory_space=pltpu.HBM)
    return pl.pallas_call(
        functools.partial(layer_kernel, chain, teams, scale, rope_dim),
        out_shape=pltpu.VMEM((part, model), bf16),
        in_specs=[hbm] * 15,
        out_specs=vmem,
        scratch_shapes=[
            pltpu.VMEM((row_count, head_count * head_dim), bf16),
            pltpu.VMEM((lanes, row_count), bf16),
            pltpu.VMEM((row_count, rank), bf16),
            pltpu.VMEM((rope_dim, row_count), bf16),
            pltpu.VMEM((1, rank), f32),
            pltpu.VMEM((1, lanes), f32),
            pltpu.VMEM(key_up.shape, bf16),
            pltpu.VMEM(value_up.shape, bf16),
            pltpu.VMEM((part, model), bf16),
            pltpu.VMEM((1, model), f32),
            pltpu.VMEM((1, model), f32),
            pltpu.VMEM((head_count, row_count, head_dim + lanes), bf16),
            pltpu.VMEM((chain, 2, teams, part, width), bf16),
            pltpu.VMEM((chain, 2, deep, half_hidden), bf16),
            pltpu.VMEM((chain, 2, deep, half_hidden), bf16),
            pltpu.VMEM((chain, 2, half_hidden, slim), bf16),
            pltpu.VMEM((2,) + out_proj.shape, bf16),
            pltpu.VMEM((2, teams // 2, part, head_count * head_dim), bf16),
            pltpu.VMEM((2, teams // 2, part, head_count * head_dim), bf16),
            pltpu.VMEM((chunks, teams // 2, part, model // chunks), bf16),
            pltpu.VMEM((chunks, teams // 2, part, model // chunks), bf16),
            pltpu.VMEM((group, part, model), bf16),
            pltpu.VMEM((group, part, half_hidden), bf16),
            pltpu.VMEM((chain, teams // 2, 2, part, 2 * slim), bf16),
            pltpu.VMEM((chain, teams // 2, 2, part, 2 * slim), bf16),
            pltpu.VMEM((chain, teams // 2, 2, part, 2 * slim), bf16),
            pltpu.VMEM((chain, teams // 2, 2, part // 2, 2 * slim), bf16),
            pltpu.VMEM((chain, teams // 2, part // 2, 2 * slim), bf16),
            pltpu.VMEM((chain, teams // 2, part // 2, 2 * slim), bf16),
            pltpu.VMEM((chain, part // 2, 2 * slim), bf16),
            pltpu.VMEM((chain, teams // 2, part // 2, 2 * slim), bf16),
            pltpu.VMEM((chain, part // 2, 2 * slim), bf16),
            pltpu.VMEM((part, model), f32),
            pltpu.VMEM((head_count, row_count, 1), f32),
            pltpu.VMEM((head_count, row_count, 1), f32),
            pltpu.VMEM((head_count, row_count, head_dim), f32),
            dma((11,)),
            dma((5,)),
            dma((chain, 2, teams)),
            dma((chain,)),
            dma((chain,)),
            dma((chain, teams // 2 - 1)),
            dma((chain,)),
            dma((chain, 2, teams // 2 - 1)),
            dma((chain, 2, teams // 2)),
            dma((3, chain, 2)),
            dma((3, chain)),
            dma((3, chain)),
            dma((2,)),
            dma((2,)),
            dma((chunks, teams // 2 - 1)),
            dma((chunks, teams // 2 - 1)),
            dma((2, stages)),
            dma((2, stages)),
            dma((chain,)),
            dma((chain,)),
            dma((chain, 2, teams // 2)),
            dma((chain, 2, teams // 2)),
        ],
        compiler_params=pltpu.CompilerParams(
            collective_id=0, has_side_effects=True, vmem_limit_bytes=60 * 1024 * 1024
        ),
    )(
        queries_nope.reshape(row_count, head_count * head_dim),
        queries_rope.transpose(1, 2, 0).reshape(lanes, row_count),
        latent,
        rope_key.T,
        latent_gain.reshape(1, -1),
        rates,
        key_up,
        value_up,
        out_proj,
        stream,
        mix_gain.reshape(1, -1),
        w_gate,
        w_up,
        w_down,
        mlp_gain.reshape(1, -1),
    )


def solution(mesh):
    return jax.shard_map(
        functools.partial(per_device, mesh.shape["sp"] // 2, mesh.shape["tp"]),
        mesh=mesh,
        in_specs=(
            P("sp", "tp", None),
            P("sp", "tp", None),
            P("sp", None),
            P("sp", None),
            P(),
            P(None, "tp"),
            P(None, "tp"),
            P("tp", None),
            P(("sp", "tp"), None),
            P(),
            P("sp", "tp"),
            P("sp", "tp"),
            P("tp", "sp"),
            P(),
        ),
        out_specs=P(("sp", "tp"), None),
        check_vma=False,
    )
```

```python
import functools
import math

import jax
import jax.numpy as jnp
import numpy as np
from jax import lax
from jax.experimental import pallas as pl
from jax.experimental.pallas import tpu as pltpu
from jax.sharding import PartitionSpec as P

theta_base = 10000.0
residual_weight = 8.0**0.25
norm_floor = 1.0
big_negative = -1e30


def latent_norm(latent, latent_gain):
    wide = latent.astype(jnp.float32)
    factor = lax.rsqrt(jnp.mean(wide * wide, axis=-1, keepdims=True) + norm_floor)
    return (wide * factor * latent_gain).astype(jnp.bfloat16)


def layer_norm(values, gain):
    centre = jnp.mean(values, axis=-1, keepdims=True)
    centred = values - centre
    spread = jnp.mean(centred * centred, axis=-1, keepdims=True)
    return centred * lax.rsqrt(spread + norm_floor) * gain


mesh_id = pl.DeviceIdType.MESH
bf16 = jnp.bfloat16
f32 = jnp.float32


def layer_kernel(
    chain,
    teams,
    scale,
    rope_dim,
    nope_hbm,
    rope_hbm,
    latent_hbm,
    rope_key_hbm,
    latent_gain_hbm,
    rates_hbm,
    key_up_hbm,
    value_up_hbm,
    proj_in,
    stream_hbm,
    mix_gain_hbm,
    gate_in,
    up_in,
    down_in,
    mlp_gain_hbm,
    result,
    nope,
    rope,
    latent_in,
    rope_key,
    latent_gain,
    rates,
    key_up,
    value_up,
    stream,
    mix_gain,
    mlp_gain,
    qcat,
    value_turned,
    lat,
    gate,
    up,
    down,
    proj,
    heads_out,
    heads_in,
    share_out,
    share_in,
    rows,
    hidden,
    terms_out,
    mate_in,
    terms,
    x_first,
    z_first,
    x_relay,
    z_relay,
    x_last,
    z_last,
    lowered,
    wide,
    top,
    total,
    weighted,
    load_sem,
    local_sem,
    lat_recv,
    lat_z,
    lat_y,
    lat_w,
    lat_next,
    lat_x,
    lat_m,
    w_recv,
    w_z,
    w_y,
    core_recv,
    core_send,
    share_recv,
    share_send,
    row_recv,
    row_send,
    mate_recv,
    mate_send,
    term_recv,
    term_send,
):
    sp = lax.axis_index("sp")
    t = lax.axis_index("tp")
    q = sp // 2
    p = sp % 2
    other = 1 - p
    half = t % 2
    column = t // 2
    columns = teams // 2
    mate = t + 1 - 2 * half
    layer = q % 2
    group = 2 * teams
    mine = half * teams + column * 2 + layer
    last = chain - 1
    head_count = qcat.shape[0]
    head_dim = value_up.shape[1] // head_count
    block_rows = qcat.shape[1]
    width = value_up.shape[0]
    part = block_rows // teams

    def place(pp, tt, qq=None):
        return ((q if qq is None else qq) * 2 + pp, tt)

    def across(step):
        return lax.rem(t + step, teams)

    def remote(source, target, send, recv, device):
        return pltpu.make_async_remote_copy(
            src_ref=source,
            dst_ref=target,
            send_sem=send,
            recv_sem=recv,
            device_id=device,
            device_id_type=mesh_id,
        )

    def pair_place(zz, tt):
        return place(p, tt, q - layer + zz)

    far_steps = range(2, teams, 2)
    barrier = pltpu.get_barrier_semaphore()
    peers = [place(p, t, lax.rem(q + d, chain)) for d in range(1, chain)]
    peers += [place(other, t), place(p, mate)]
    peers += [place(p, across(step)) for step in far_steps]
    peers += [pair_place(1 - layer, across(step)) for step in far_steps]
    for device in peers:
        pl.semaphore_signal(barrier, inc=1, device_id=device, device_id_type=mesh_id)

    loads = [
        pltpu.make_async_copy(source, target, load_sem.at[i])
        for i, (source, target) in enumerate(
            (
                (latent_hbm, latent_in),
                (rope_key_hbm, rope_key),
                (latent_gain_hbm, latent_gain),
                (rates_hbm, rates),
                (rope_hbm, rope),
                (nope_hbm, nope),
                (key_up_hbm, key_up),
                (value_up_hbm, value_up),
                (stream_hbm, stream),
                (mix_gain_hbm, mix_gain),
                (mlp_gain_hbm, mlp_gain),
            )
        )
    ]
    for load in loads:
        load.start()

    def lat_to_z(qq):
        return remote(
            lat.at[q, p, t], lat.at[q, p, t], lat_z.at[qq], lat_recv.at[q, p, t], place(p, t, qq)
        )

    def lat_to_next(j):
        spot = lat.at[j, p, t]
        return remote(spot, spot, lat_next.at[j], lat_recv.at[j, p, t], place(p, t, q + 1))

    def lat_side(j, step):
        spot = lat.at[j, p, across(step)]
        return remote(
            spot, spot, lat_w.at[j, step // 2 - 1], lat_recv.at[j, p, across(step)], place(other, t)
        )

    def turned(j):
        return (j % 2 == 1) & (j < q)

    def lat_own_y():
        return remote(
            lat.at[q, p, t], lat.at[q, p, t], lat_y.at[q], lat_recv.at[q, p, t], place(other, t)
        )

    def lat_to_y(j):
        spot = lat.at[j, p, t]
        return remote(spot, spot, lat_y.at[j], lat_recv.at[j, p, t], place(other, t))

    def lat_to_x(j, pp, step):
        spot = lat.at[j, pp, t]
        return remote(
            spot, spot, lat_x.at[j, pp, step // 2 - 1], lat_recv.at[j, pp, t], place(p, across(step))
        )

    def lat_to_m(j, pp, tt):
        spot = lat.at[j, pp, tt]
        return remote(spot, spot, lat_m.at[j, pp, tt // 2], lat_recv.at[j, pp, tt], place(p, mate))

    def lat_wait(j, pp, tt):
        spot = lat.at[j, pp, tt]
        with jax.named_scope("lat_wait"):
            remote(spot, spot, lat_y.at[0], lat_recv.at[j, pp, tt], place(p, mate)).wait_recv()

    stores = (gate, up, down)
    hidden_half = gate.shape[3]

    def piece(w, which):
        start = pl.multiple_of(which * hidden_half, 128)
        if w == 0:
            return gate_in.at[:, pl.ds(start, hidden_half)]
        if w == 1:
            return up_in.at[:, pl.ds(start, hidden_half)]
        return down_in.at[pl.ds(start, hidden_half), :]

    def w_to_z(w, qq):
        return remote(
            piece(w, qq % 2),
            stores[w].at[q, p],
            w_z.at[w, qq],
            w_recv.at[w, q, p],
            place(p, t, qq),
        )

    def w_own_y(w):
        return remote(
            piece(w, layer), stores[w].at[q, p], w_y.at[w, q], w_recv.at[w, q, p], place(other, t)
        )

    def w_to_y(w, j):
        spot = stores[w].at[j, p]
        return remote(spot, spot, w_y.at[w, j], w_recv.at[w, j, p], place(other, t))

    def w_wait(w, j, pp):
        spot = stores[w].at[j, pp]
        with jax.named_scope("w_wait"):
            remote(spot, spot, w_y.at[w, 0], w_recv.at[w, j, pp], place(p, mate)).wait_recv()

    def w_own(w):
        return pltpu.make_async_copy(piece(w, layer), stores[w].at[q, p], local_sem.at[1 + w])

    own_proj = pltpu.make_async_copy(proj_in, proj.at[half], local_sem.at[4])
    proj_mate = remote(proj_in, proj.at[half], core_send.at[0], core_recv.at[0], place(p, mate))

    beyond = range(2, chain)

    def lat_own_to_z(act):
        for d in range(1, chain):

            takes = (q + d <= last) & (((q + d) % 2 == 0) | ((d == 1) & (layer == 0)))

            @pl.when(takes)
            def _():
                act(lat_to_z(q + d))

    def toward(w, near, act):
        for d in (1,) if near else range(2, chain) if w == 2 else range(last, 1, -1):

            @pl.when((layer == 0) & (q + d <= last))
            def _():
                act(w_to_z(w, q + d))

            @pl.when((layer == 1) & (q - d >= 0))
            def _():
                act(w_to_z(w, q - d))

    def away(w, distances, act):
        for d in distances:

            @pl.when((layer == 1) & (q + d <= last))
            def _():
                act(w_to_z(w, q + d))

            @pl.when((layer == 0) & (q - d >= 0))
            def _():
                act(w_to_z(w, q - d))

    def start(copy):
        copy.start()

    def sent(copy):
        copy.wait_send()

    for w in range(3):
        w_own(w).start()
    own_proj.start()

    lanes = head_count * rope_dim
    turn_rows = lax.broadcasted_iota(jnp.int32, (block_rows, lanes), 0)
    turn_lanes = lax.broadcasted_iota(jnp.int32, (block_rows, lanes), 1)
    left = lax.rem(turn_lanes, rope_dim) < rope_dim // 2
    loads[3].wait()
    with jax.named_scope("angles"):
        angle = (sp * block_rows + turn_rows).astype(f32) * rates[...]
        cosine = jnp.cos(angle)
        sine = jnp.sin(angle)
        sine = jnp.where(left, -sine, sine)

    def turn(vector):
        ahead = pltpu.roll(vector, lanes - rope_dim // 2, 1)
        behind = pltpu.roll(vector, rope_dim // 2, 1)
        return vector * cosine + jnp.where(left, ahead, behind) * sine

    def alone(vector):
        return jnp.where(turn_lanes < rope_dim, vector, 0.0).astype(bf16)

    for load in loads[:3]:
        load.wait()
    with jax.named_scope("latent"):
        lat[q, p, :, :, :width] = latent_norm(latent_in[...], latent_gain[...]).reshape(
            teams, part, width
        )
        key = rope_key[...].astype(f32)
        key = turn(jnp.concatenate([key] * head_count, axis=0).T)
        lat[q, p, :, :, width:] = alone(key).reshape(teams, part, lanes)
    with jax.named_scope("barrier"):
        pl.semaphore_wait(barrier, len(peers))
    lat_own_to_z(start)

    @pl.when(p == 0)
    def _():
        lat_own_y().start()

    w_own_y(0).start()
    patient = q == last - 1

    def all_toward():
        toward(0, True, start)

        @pl.when(layer == 0)
        def _():
            toward(1, True, start)

            @pl.when(jnp.logical_not(patient))
            def _():
                toward(2, True, start)

        toward(0, False, start)
        toward(1, False, start)

        @pl.when(layer == 1)
        def _():
            toward(1, True, start)
            toward(2, True, start)

    for w, distances in ((0, (1,)), (0, beyond), (1, (1,)), (1, beyond), (2, (1,))):
        away(w, distances, start)

    @pl.when(jnp.logical_not(patient))
    def _():
        all_toward()

    proj_mate.start()
    for load in loads[4:6]:
        load.wait()
    nope_wide = nope[...].astype(f32)
    turned_queries = turn(rope[...].astype(f32).T)
    for h in range(head_count):
        qcat[h, :, :head_dim] = nope_wide[:, h, :].astype(bf16)
        shifted = turned_queries if h == 0 else pltpu.roll(turned_queries, lanes - h * rope_dim, 1)
        qcat[h, :, head_dim:] = alone(shifted)

    top[...] = jnp.full_like(top, big_negative)
    total[...] = jnp.zeros_like(total)
    weighted[...] = jnp.zeros_like(weighted)

    def attend(j, pp, diagonal):
        block = lat[j, pp].reshape(block_rows, lat.shape[4])
        normed = block[:, :width]
        rotary = block[:, width:]
        keys = jnp.dot(normed, key_up[...], preferred_element_type=f32).astype(bf16)
        values = lax.dot_general(
            value_turned[...], normed, (((1,), (1,)), ((), ())), preferred_element_type=f32
        ).astype(bf16)
        for h in range(head_count):
            span = slice(h * head_dim, (h + 1) * head_dim)
            both = jnp.concatenate([keys[:, span], rotary], axis=1)
            score = lax.dot_general(
                both, qcat[h], (((1,), (1,)), ((), ())), preferred_element_type=f32
            )
            if diagonal:
                source_rows = lax.broadcasted_iota(jnp.int32, score.shape, 0)
                query_rows = lax.broadcasted_iota(jnp.int32, score.shape, 1)
                score = jnp.where(source_rows <= query_rows, score, big_negative)
            old = top[h]
            new = jnp.maximum(old, jnp.max(score, axis=0, keepdims=True))
            powers = jnp.exp2(score * scale - new * scale)
            shrink = jnp.exp2((old - new) * scale)
            total[h] = total[h] * shrink + jnp.sum(powers, axis=0, keepdims=True)
            weighted[h] = weighted[h] * shrink + jnp.dot(
                values[span], powers.astype(bf16), preferred_element_type=f32
            )
            top[h] = new

    for load in loads[6:]:
        load.wait()
    value_turned[...] = value_up[...].astype(f32).T.astype(bf16)
    with jax.named_scope("attend_own"):
        attend(q, p, True)

    own = "own"

    def is_edge(j):
        return (j % 4 == 0) | (j % 4 == 3)

    def forward(w, kind):
        for j in range(chain):
            distant = q // 2 != j // 2
            if kind == 1:
                takes = (q // 2 == j // 2) & (q != j)
            elif is_edge(j) == (kind == 0):
                takes = distant
            else:
                continue

            @pl.when(takes)
            def _():
                w_wait(w, j, p)
                w_to_y(w, j).start()

    plans = {
        "early": (((0, 1),), ((0, 2), (0, 1)), ((0, 1),), ()),
        "late": (((0, 0), (1, 1)), ((0, 0), (1, 1)), ((0, 2),), ((0, 2),)),
        "after": ((), (), (own,), ((0, 0),)),
        "share": (((1, 0), own, (2, 1)), ((1, 0),), ((1, 1),), ((0, 1),)),
        "half": ((), (), (), ((1, 0), (1, 1))),
        "rows": ((), ((1, 2), own, (2, 1)), ((0, 0), (1, 0), (1, 2)), ((1, 2), own)),
        "near": (((0, 2),), (), ((2, 1),), ()),
        "middle": (((1, 2),), (), (), ()),
        "far": ((), (), ((2, 2),), ()),
        "last": (((2, 2),), ((2, 2),), ((2, 0),), ()),
        "end": ((), (), (), ((2, 0),)),
        "first": ((), (), (), ((2, 2), (2, 1))),
        "second": (((2, 0),), ((2, 0),), (), ()),
    }

    def pass_along(name):
        for kind_of, plan in enumerate(plans[name]):
            if plan:

                @pl.when(q % 4 == kind_of)
                def _():
                    for entry in plan:
                        if entry is own:
                            w_own_y(2).start()
                        else:
                            forward(*entry)

    def lat_step(s, carry):
        a = q - s

        @pl.when(a >= 0)
        def _():
            lat_wait(a, p, t)
            lat_to_y(a).start()
            for step in far_steps:
                lat_to_x(a, p, step).start()
            lat_to_m(a, p, t).start()

            @pl.when(layer == 0)
            def _():
                lat_to_next(a).start()

        b = q - s + 1

        @pl.when((b >= 0) & ((s >= 2) | (p == 1)))
        def _():
            lat_wait(b, other, t)

            @pl.when(jnp.logical_not(turned(b)))
            def _():
                for step in far_steps:
                    lat_to_x(b, other, step).start()

            lat_to_m(b, other, t).start()

        @pl.when(s == 3)
        def _():
            w_own_y(1).start()

        @pl.when((s == 3) & patient)
        def _():
            all_toward()

        def block(j, pp):
            for i in range(columns):
                lat_wait(j, pp, 2 * i + 1 - half)
            with jax.named_scope("attend"):
                attend(j, pp, False)

        def stage(k, inner):
            e = q - s + 2 + k

            @pl.when((e >= 0) & ((s >= 4) | ((s == 3) & ((k == 0) | (p == 1)))))
            def _():
                block(e, jnp.where(k == 0, p, other))

            c = b + k
            side = jnp.where(k == 0, p, other)
            ready = (s >= 2) & ((k == 0) | (s >= 3) | (p == 1))

            @pl.when((c >= 0) & ready)
            def _():
                for step in far_steps:
                    lat_wait(c, side, across(step))

                    @pl.when(turned(c) & (k == 0))
                    def _():
                        lat_side(c, step).start()

                    lat_to_m(c, side, across(step)).start()

            return inner

        lax.fori_loop(0, 2, stage, 0)
        for turn, name in ((4, "early"), (5, "late")):

            @pl.when(s == turn)
            def _():
                pass_along(name)

        return carry

    lax.fori_loop(1, max(chain + 3, 6), lat_step, 0)
    pass_along("after")


    for h in range(head_count):
        span = slice(h * head_dim, (h + 1) * head_dim)
        done = (weighted[h] / total[h]).T.astype(bf16)
        done = done.reshape(teams, part, head_dim)
        for tt in range(teams):
            heads_out[tt % 2, tt // 2, :, span] = done[tt]

    heads_mate = remote(
        heads_out.at[1 - half], heads_in.at[half], core_send.at[1], core_recv.at[1], place(p, mate)
    )
    heads_mate.start()
    heads_in[half] = heads_out[half]
    own_proj.wait()
    for w in range(3):
        w_own(w).wait()
    with jax.named_scope("head_wait"):
        proj_mate.wait_recv()
        heads_mate.wait_recv()

    chunks = share_out.shape[0]
    span_share = share_out.shape[3]

    def project(i, c):
        span = slice(c * span_share, (c + 1) * span_share)
        return jnp.dot(
            heads_in[0, i], proj[0, :, span], preferred_element_type=f32
        ) + jnp.dot(heads_in[1, i], proj[1, :, span], preferred_element_type=f32)

    def share_to(c, step):
        i = lax.rem(column + step, columns)
        return remote(
            share_out.at[c, i],
            share_in.at[c, column],
            share_send.at[c, step - 1],
            share_recv.at[c, step - 1],
            place(p, 2 * i + half),
        )

    with jax.named_scope("project"):
        for c in range(chunks):
            for step in range(1, columns):
                i = lax.rem(column + step, columns)
                share_out[c, i] = project(i, c).astype(bf16)
                share_to(c, step).start()
        pass_along("share")
        for c in range(chunks):
            span = slice(c * span_share, (c + 1) * span_share)
            wide[:, span] = residual_weight * stream[:, span].astype(f32) + project(column, c)
    for c in range(chunks):
        span = slice(c * span_share, (c + 1) * span_share)
        for step in range(1, columns):
            with jax.named_scope("share_wait"):
                share_to(c, step).wait_recv()
            source = lax.rem(column - step + columns, columns)
            wide[:, span] += share_in[c, source].astype(f32)
        if c == 0:
            pass_along("half")
    with jax.named_scope("norm"):
        rows[mine] = layer_norm(wide[...], mix_gain[...]).astype(bf16)

    bits = []
    bit = 2
    while bit < teams:
        bits.append(bit)
        bit *= 2
    orders = (bits + [0, 1], [0] + bits + [1])
    depth = len(orders[0])
    sub = part // 2

    def flip(stage, zz, tt):
        if stage == 0:
            return 1 - zz, tt
        return zz, jnp.where((tt // stage) % 2 == 0, tt + stage, tt - stage)

    holdings = []
    for order in orders:
        held = [(layer, t)]
        for stage in order:
            held = held + [flip(stage, zz, tt) for zz, tt in held]
        holdings.append(held)

    def row_copy(o, i, u):
        zz, tt = holdings[o][u]
        index = (tt % 2) * teams + (tt // 2) * 2 + zz
        spot = rows.at[index, pl.ds(o * sub, sub)]
        slot = 2**i - 1 + u
        partner = pair_place(*flip(orders[o][i], layer, t))
        return remote(spot, spot, row_send.at[o, slot], row_recv.at[o, slot], partner)

    for i in range(depth):
        for o in range(2):
            row_copy(o, i, 0).start()
    pass_along("rows")
    def row_stage(i):
        for o in range(2):
            for u in range(2**i):
                with jax.named_scope("row_wait"):
                    row_copy(o, i, u).wait_recv()
                for later in range(i + 1, depth):
                    row_copy(o, later, 2**i + u).start()

    def feed(k, carry):
        here = rows[pl.ds(2 * k, 2)].reshape(2 * part, rows.shape[2])
        gate_sum = jnp.dot(
            here, gate[...].reshape(-1, hidden_half), preferred_element_type=f32
        )
        up_sum = jnp.dot(here, up[...].reshape(-1, hidden_half), preferred_element_type=f32)
        value = gate_sum / (1.0 + jnp.exp(-gate_sum)) * up_sum
        hidden[pl.ds(2 * k, 2)] = value.astype(bf16).reshape(2, part, hidden_half)
        return carry

    for i in range(depth - 1):
        row_stage(i)
        if i == 0:
            pass_along("near")

            toward(2, False, start)

            @pl.when(patient)
            def _():
                toward(2, True, start)

            @pl.when(layer == 0)
            def _():
                away(2, beyond, start)

            pass_along("middle")
    pass_along("far")
    for w in range(2):
        for j in range(chain):
            w_wait(w, j, other)
    with jax.named_scope("feed"):
        lax.fori_loop(half * columns, half * columns + columns, feed, 0)

    @pl.when(layer == 1)
    def _():
        away(2, beyond, start)

    pass_along("last")
    row_stage(depth - 1)
    with jax.named_scope("feed"):
        lax.fori_loop((1 - half) * columns, (1 - half) * columns + columns, feed, 0)
    pass_along("end")

    def settle(j, carry):
        @pl.when(j != q)
        def _():
            for w in range(2):
                w_to_y(w, j).wait_send()

        @pl.when(j < q)
        def _():
            lat_to_y(j).wait_send()

            @pl.when(layer == 0)
            def _():
                lat_to_next(j).wait_send()

            for step in far_steps:
                lat_to_x(j, p, step).wait_send()

                @pl.when(turned(j))
                def _():
                    lat_side(j, step).wait_send()

            for i in range(columns):
                lat_to_m(j, p, 2 * i + half).wait_send()

        @pl.when((j < q) | ((j == q) & (p == 1)))
        def _():
            @pl.when(jnp.logical_not(turned(j)))
            def _():
                for step in far_steps:
                    lat_to_x(j, other, step).wait_send()

            for i in range(columns):
                lat_to_m(j, other, 2 * i + half).wait_send()

        return carry

    with jax.named_scope("settle"):
        proj_mate.wait_send()
        heads_mate.wait_send()
        for c in range(chunks):
            for step in range(1, columns):
                share_to(c, step).wait_send()

        @pl.when(p == 0)
        def _():
            lat_own_y().wait_send()

        lax.fori_loop(0, chain, settle, 0)
        lat_own_to_z(sent)
        for w in range(2):
            w_own_y(w).wait_send()
            toward(w, False, sent)
            toward(w, True, sent)
            away(w, range(1, chain), sent)

    def block_at(n):
        here = q // 2
        upper = here % 2
        skip = 2 - upper
        ahead = jnp.maximum(n - skip, 0)
        there = lax.rem(here + 1 + ahead // 2, chain // 2)
        edge = 2 * there + there % 2
        distant = jnp.where((ahead + upper) % 2 == 1, edge, 4 * there + 1 - edge)
        own_edge = 2 * here + upper
        own_inner = 4 * here + 1 - own_edge
        chosen = jnp.where(n == 0, own_edge, jnp.where(n < skip, own_inner, distant))
        return jnp.where((upper == 1) & (n == chain - 1), own_inner, chosen)

    def term_mate(j):
        return remote(
            terms_out.at[j], mate_in.at[j], mate_send.at[j], mate_recv.at[j], place(p, mate)
        )

    def term_x(j, step):
        i = lax.rem(column + step, columns)
        return remote(
            terms.at[j, i, :, pl.ds(0, sub)],
            x_first.at[j, column],
            term_send.at[j, 0, step],
            term_recv.at[j, 0, step],
            place(p, 2 * i + half),
        )

    def term_z(j):
        return remote(
            terms.at[j, :, 1 - layer, pl.ds(sub, sub)],
            z_first.at[j],
            term_send.at[j, 1, 0],
            term_recv.at[j, 1, 0],
            pair_place(1 - layer, t),
        )

    def relay_x(j, step):
        i = lax.rem(column + step, columns)
        return remote(
            x_relay.at[j, i],
            x_last.at[j, column],
            term_send.at[j, 1, step],
            term_recv.at[j, 1, step],
            place(p, 2 * i + half),
        )

    def relay_z(j):
        return remote(
            z_relay.at[j],
            z_last.at[j],
            term_send.at[j, 0, 0],
            term_recv.at[j, 0, 0],
            pair_place(1 - layer, t),
        )

    own_rows = half * teams

    def product(j, first):
        weights = jnp.concatenate([down[j, 0], down[j, 1]], axis=1)
        here = hidden[pl.ds(first, teams)].reshape(teams * part, hidden_half)
        out = jnp.dot(here, weights, preferred_element_type=f32)
        return out.reshape(columns, 2, part, out.shape[1])

    def lower_mate(j):
        terms_out[j] = product(j, teams - own_rows).astype(bf16)
        term_mate(j).start()

    def lower_own(j):
        kept = product(j, own_rows)
        with jax.named_scope("mate_wait"):
            term_mate(j).wait_recv()
        terms[j] = (kept + mate_in[j].astype(f32)).astype(bf16)
        for step in range(1, columns):
            term_x(j, step).start()
        term_z(j).start()

    def sources():
        return [lax.rem(column - step + columns, columns) for step in range(1, columns)]

    def relay(j):
        with jax.named_scope("relay_wait"):
            for step in range(1, columns):
                term_x(j, step).wait_recv()
            term_z(j).wait_recv()
        far = terms[j, column, 1 - layer, :sub].astype(f32)
        for source in sources():
            far = far + x_first[j, source, 1 - layer].astype(f32)
        z_relay[j] = far.astype(bf16)
        relay_z(j).start()
        for step in range(1, columns):
            i = lax.rem(column + step, columns)
            side = terms[j, i, layer, sub:].astype(f32) + z_first[j, i].astype(f32)
            x_relay[j, i] = side.astype(bf16)
            relay_x(j, step).start()

    span_width = terms.shape[4]

    def finish(j):
        with jax.named_scope("term_wait"):
            relay_z(j).wait_recv()
            for step in range(1, columns):
                relay_x(j, step).wait_recv()
        top_rows = terms[j, column, layer, :sub].astype(f32) + z_last[j].astype(f32)
        low_rows = terms[j, column, layer, sub:].astype(f32) + z_first[j, column].astype(f32)
        for source in sources():
            top_rows = top_rows + x_first[j, source, layer].astype(f32)
            low_rows = low_rows + x_last[j, source].astype(f32)
        lowered[j, :sub] = top_rows
        lowered[j, sub:] = low_rows

    def lower_step(n, carry):
        @pl.when(n < chain)
        def _():
            j = block_at(n)
            w_wait(2, j, other)
            with jax.named_scope("lower_mate"):
                lower_mate(j)
            with jax.named_scope("lower_own"):
                lower_own(j)

        for turn, name in ((0, "first"), (1, "second")):

            @pl.when(n == turn)
            def _():
                pass_along(name)

        @pl.when((n >= 1) & (n <= chain))
        def _():
            relay(block_at(n - 1))

        @pl.when(n >= 2)
        def _():
            finish(block_at(n - 2))

        return carry

    lax.fori_loop(0, chain + 2, lower_step, 0)
    for j in range(chain):
        span = slice(j * span_width, (j + 1) * span_width)
        kept_rows = residual_weight * rows[mine, :, span].astype(f32)
        wide[:, span] = kept_rows + 0.5 * lowered[j]
    with jax.named_scope("norm"):
        result[...] = layer_norm(wide[...], mlp_gain[...]).astype(bf16)

    for o in range(2):
        for i in range(depth):
            for u in range(2**i):
                row_copy(o, i, u).wait_send()
    w_own_y(2).wait_send()
    toward(2, False, sent)
    toward(2, True, sent)
    away(2, range(1, chain), sent)

    def drain(j, carry):
        term_mate(j).wait_send()
        term_z(j).wait_send()
        relay_z(j).wait_send()
        for step in range(1, columns):
            term_x(j, step).wait_send()
            relay_x(j, step).wait_send()

        @pl.when(j != q)
        def _():
            w_to_y(2, j).wait_send()

        return carry

    with jax.named_scope("drain"):
        lax.fori_loop(0, chain, drain, 0)


def per_device(
    chain,
    teams,
    queries_nope,
    queries_rope,
    latent,
    rope_key,
    latent_gain,
    key_up,
    value_up,
    out_proj,
    stream,
    mix_gain,
    w_gate,
    w_up,
    w_down,
    mlp_gain,
):
    row_count, head_count, head_dim = queries_nope.shape
    rope_dim = queries_rope.shape[2]
    scale = (head_dim + rope_dim) ** (-0.5) * math.log2(math.e)
    lanes = head_count * rope_dim
    half_rope = rope_dim // 2
    rates = theta_base ** (-2.0 * (np.arange(lanes) % half_rope) / rope_dim)
    rates = jnp.asarray(rates, f32).reshape(1, lanes)
    rank = latent.shape[1]
    width = rank + lanes
    model, hidden_here = w_gate.shape[0] * 2 * chain, w_gate.shape[1]
    group = 2 * teams
    part = row_count // teams
    half_hidden = hidden_here // 2
    deep = w_gate.shape[0]
    slim = w_down.shape[1]
    stages = group - 1
    chunks = 4
    dma = pltpu.SemaphoreType.DMA
    vmem = pl.BlockSpec(memory_space=pltpu.VMEM)
    hbm = pl.BlockSpec(memory_space=pltpu.HBM)
    return pl.pallas_call(
        functools.partial(layer_kernel, chain, teams, scale, rope_dim),
        out_shape=pltpu.VMEM((part, model), bf16),
        in_specs=[hbm] * 15,
        out_specs=vmem,
        scratch_shapes=[
            pltpu.VMEM(queries_nope.shape, bf16),
            pltpu.VMEM((lanes, row_count), bf16),
            pltpu.VMEM((row_count, rank), bf16),
            pltpu.VMEM((rope_dim, row_count), bf16),
            pltpu.VMEM((1, rank), f32),
            pltpu.VMEM((1, lanes), f32),
            pltpu.VMEM(key_up.shape, bf16),
            pltpu.VMEM(value_up.shape, bf16),
            pltpu.VMEM((part, model), bf16),
            pltpu.VMEM((1, model), f32),
            pltpu.VMEM((1, model), f32),
            pltpu.VMEM((head_count, row_count, head_dim + lanes), bf16),
            pltpu.VMEM((value_up.shape[1], value_up.shape[0]), bf16),
            pltpu.VMEM((chain, 2, teams, part, width), bf16),
            pltpu.VMEM((chain, 2, deep, half_hidden), bf16),
            pltpu.VMEM((chain, 2, deep, half_hidden), bf16),
            pltpu.VMEM((chain, 2, half_hidden, slim), bf16),
            pltpu.VMEM((2,) + out_proj.shape, bf16),
            pltpu.VMEM((2, teams // 2, part, head_count * head_dim), bf16),
            pltpu.VMEM((2, teams // 2, part, head_count * head_dim), bf16),
            pltpu.VMEM((chunks, teams // 2, part, model // chunks), bf16),
            pltpu.VMEM((chunks, teams // 2, part, model // chunks), bf16),
            pltpu.VMEM((group, part, model), bf16),
            pltpu.VMEM((group, part, half_hidden), bf16),
            pltpu.VMEM((chain, teams // 2, 2, part, 2 * slim), bf16),
            pltpu.VMEM((chain, teams // 2, 2, part, 2 * slim), bf16),
            pltpu.VMEM((chain, teams // 2, 2, part, 2 * slim), bf16),
            pltpu.VMEM((chain, teams // 2, 2, part // 2, 2 * slim), bf16),
            pltpu.VMEM((chain, teams // 2, part // 2, 2 * slim), bf16),
            pltpu.VMEM((chain, teams // 2, part // 2, 2 * slim), bf16),
            pltpu.VMEM((chain, part // 2, 2 * slim), bf16),
            pltpu.VMEM((chain, teams // 2, part // 2, 2 * slim), bf16),
            pltpu.VMEM((chain, part // 2, 2 * slim), bf16),
            pltpu.VMEM((chain, part, 2 * slim), f32),
            pltpu.VMEM((part, model), f32),
            pltpu.VMEM((head_count, 1, row_count), f32),
            pltpu.VMEM((head_count, 1, row_count), f32),
            pltpu.VMEM((head_count, head_dim, row_count), f32),
            dma((11,)),
            dma((5,)),
            dma((chain, 2, teams)),
            dma((chain,)),
            dma((chain,)),
            dma((chain, teams // 2 - 1)),
            dma((chain,)),
            dma((chain, 2, teams // 2 - 1)),
            dma((chain, 2, teams // 2)),
            dma((3, chain, 2)),
            dma((3, chain)),
            dma((3, chain)),
            dma((2,)),
            dma((2,)),
            dma((chunks, teams // 2 - 1)),
            dma((chunks, teams // 2 - 1)),
            dma((2, stages)),
            dma((2, stages)),
            dma((chain,)),
            dma((chain,)),
            dma((chain, 2, teams // 2)),
            dma((chain, 2, teams // 2)),
        ],
        compiler_params=pltpu.CompilerParams(
            collective_id=0, has_side_effects=True, vmem_limit_bytes=60 * 1024 * 1024
        ),
    )(
        queries_nope,
        queries_rope.transpose(1, 2, 0).reshape(lanes, row_count),
        latent,
        rope_key.T,
        latent_gain.reshape(1, -1),
        rates,
        key_up,
        value_up,
        out_proj,
        stream,
        mix_gain.reshape(1, -1),
        w_gate,
        w_up,
        w_down,
        mlp_gain.reshape(1, -1),
    )


def solution(mesh):
    return jax.shard_map(
        functools.partial(per_device, mesh.shape["sp"] // 2, mesh.shape["tp"]),
        mesh=mesh,
        in_specs=(
            P("sp", "tp", None),
            P("sp", "tp", None),
            P("sp", None),
            P("sp", None),
            P(),
            P(None, "tp"),
            P(None, "tp"),
            P("tp", None),
            P(("sp", "tp"), None),
            P(),
            P("sp", "tp"),
            P("sp", "tp"),
            P("tp", "sp"),
            P(),
        ),
        out_specs=P(("sp", "tp"), None),
        check_vma=False,
    )
```
